32 devices in a mesh: sp: 8 (over z, x), tp: 4 (over y, core).
Axes of the slice: x: 2, y: 2, z: 4, core: 2. Of those that a mesh axis runs over, the one named last changes fastest.
Arguments:
- cotangent: bfloat16 [1024, 2048], P('sp'), may hold values from -6 to 6
- stream: bfloat16 [1024, 2048], P('sp'), may hold values from -6 to 6
- routes: int32 [1024, 2], P('sp'), may hold values from 0 to 3, all different within a row; in each aligned block of 128 rows (0 to 127, 128 to 255, ...) at most 96 rows name the same one
- route_weights: float32 [1024, 2], P('sp'), may hold values from 0.25 to 1
- gate_weight: bfloat16 [8, 2048, 2048], P('sp', None, 'tp'), may hold values from -0.125 to 0.125
- up_weight: bfloat16 [8, 2048, 2048], P('sp', None, 'tp'), may hold values from -0.125 to 0.125
- down_weight: bfloat16 [8, 2048, 2048], P('sp', 'tp'), may hold values from -0.09375 to 0.09375
- outer_gate: bfloat16 [1024, 1024], P('sp', 'tp'), may hold values from -6 to 6
- inner_gate: bfloat16 [1024, 1024], P('sp', 'tp'), may hold values from -6 to 6
- conv_input: bfloat16 [1024, 1024], P('sp', 'tp'), may hold values from -6 to 6
- conv_taps: bfloat16 [3, 1024], P(None, 'tp'), may hold values from -1 to 1
- out_weight: bfloat16 [2048, 1024], P(None, 'tp'), may hold values from -0.1875 to 0.1875
Outputs:
- gate_grad: bfloat16 [8, 2048, 2048], P('sp', None, 'tp')
- up_grad: bfloat16 [8, 2048, 2048], P('sp', None, 'tp')
- down_grad: bfloat16 [8, 2048, 2048], P('sp', 'tp')
- out_grad: float32 [2048, 1024], P('sp', 'tp')
- outer_grad: bfloat16 [1024, 1024], P('sp', 'tp')
- inner_grad: bfloat16 [1024, 1024], P('sp', 'tp')
- input_grad: bfloat16 [1024, 1024], P('sp', 'tp')
The draws below stay inside these ranges and needn't reach their ends.
Inputs may be any that keep to these rules, and one draw needn't show every extreme that they name: `routes`: each token names two different experts. Among the 128 tokens of one index of sp no expert is named by more than 96 tokens, a bound that some block of them reaches in every draw.
All inputs are finite; a program needn't handle non-finite values.
Results may differ from the reference program's by a relative error of at most 0.02.
Values may be sent and summed in bfloat16 or wider, within the bound.
A program may use at most 64 MiB of HBM per device.

```python
import math
import jax
import jax.numpy as jnp
import numpy as np
from jax import lax

D = 2048
HID = 4096
CONV = 1024
TOK_DEV = 128
HALF = 2048
CAP = 96
TOKENS = 1024
N_SP = 8
N_TP = 4


def with_spikes(entries, own_key, source, target, shards_of, factor):
    def block_of(axis_at):
        return (jnp.arange(entries.shape[axis_at]) // (entries.shape[axis_at] // shards_of)).reshape((-1,) + (1,) * (entries.ndim - 1 - axis_at))

    near = jax.random.permutation(own_key, shards_of)[block_of(target)]
    far = (block_of(target) + shards_of // 2) % shards_of
    return jnp.where((block_of(source) == near) | (block_of(source) == far), factor * entries, entries)


def block_levels(key, extent, cuts, smallest, largest):
    def one(position, parts):
        steps = jax.random.uniform(jax.random.fold_in(jax.random.fold_in(key, 6), position), (parts,), jnp.float32, smallest / len(cuts), largest / len(cuts))
        return jnp.repeat(jnp.exp(steps), extent[position] // parts).reshape((-1,) + (1,) * (len(extent) - position - 1))

    loudness = one(*cuts[0])
    for cut in cuts[1:]:
        loudness = loudness * one(*cut)
    return loudness


def routed_block(key, own, number, rows, number_of, top, most, skew):
    ranking = jax.random.permutation(key, number_of)
    crowded, ordinary = portions_of(number_of, rows * top, most, skew, True), portions_of(number_of, rows * top, most, skew, False)
    places = jnp.arange(number_of)

    def named(sizes, rotation):
        used = int((sizes > 0).sum())
        fixed = max(1, used // 4)
        shifted = fixed + (places - fixed + rotation * (used - fixed)) % max(1, number_of - fixed)
        return jnp.zeros((number_of,), jnp.int32).at[ranking[jnp.where(places < fixed, places, shifted)]].set(jnp.asarray(sizes, jnp.int32))

    sizes = jnp.where(number % 4 == 0, named(crowded, number // 4), named(ordinary, number - number // 4 - 1))
    mixed = jax.random.permutation(jax.random.fold_in(own, 3), number_of)
    donor, sink = mixed[0:number_of // 2 * 2:2], mixed[1:number_of // 2 * 2:2]
    margin = jnp.minimum(sizes[donor] - 1, most - sizes[sink]) // 2
    margin = jnp.where((donor == ranking[0]) | (sink == ranking[0]) | (sizes[sink] == 0), 0, jnp.maximum(margin, 0))
    shifted = jax.random.randint(jax.random.fold_in(own, 4), (number_of // 2,), 0, 1 << 20) % (margin + 1)
    sizes = sizes.at[donor].add(-shifted).at[sink].add(shifted)
    items = jnp.searchsorted(jnp.cumsum(sizes), jnp.arange(rows * top), side="right").astype(jnp.int32)
    grid = items.reshape(top, rows).T
    grid = grid[jax.random.permutation(jax.random.fold_in(own, 1), rows)]
    rotation = jax.random.randint(jax.random.fold_in(own, 2), (rows, 1), 0, top)
    return jnp.take_along_axis(grid, (jnp.arange(top)[None, :] + rotation) % top, axis=1)


def portions_of(count, total, reach, skew, full):
    weights = [(1 << 20) // math.isqrt(rank ** skew) + 1 for rank in range(1, count + 1)]
    largest = reach if full else min(reach, max(-(-total // count), total * weights[0] // sum(weights)))
    least = 1 if total - largest >= count - 1 else 0
    given, rest = [largest] + [least] * (count - 1), total - largest - least * (count - 1)
    while rest > 0:
        movable = [i for i in range(1, count) if given[i] < largest] or [i for i in range(1, count) if given[i] < reach]
        mass, left = sum([weights[i] for i in movable]), rest
        for i in movable:
            extra = min(reach - given[i], max(1, left * weights[i] // mass), rest)
            given[i] = given[i] + extra
            rest = rest - extra
    return np.array(given)


def scatter_about(stream_key, extent, spread, most, cuts=(), held_as=jnp.bfloat16):
    result = spread * jax.random.normal(stream_key, extent, jnp.float32)
    if cuts:
        result = result * block_levels(stream_key, extent, cuts, -0.22, 0.18)
    return jnp.clip(result, -most, most).astype(held_as)


def gaussian_with(key, shape, scale, most, pieces, heavy, kind=jnp.bfloat16):
    array = scale * jax.random.normal(key, shape, jnp.float32)
    if pieces:
        array = array * block_levels(key, shape, pieces, -0.22, 0.18)
    return jnp.clip(with_spikes(array, jax.random.fold_in(key, 3), *heavy), -most, most).astype(kind)


def setup_inputs(seed: int = 0) -> dict:
    keys = jax.random.split(jax.random.key(seed), 13)
    cotangent = gaussian_with(keys[0], (TOKENS, D), 1.0, 6.0, ((0, 8),), (0, 1, 8, 2.0))
    stream = scatter_about(keys[1], (TOKENS, D), 1.0, 6.0, ((0, 8),))
    routes_keys = jax.random.split(jax.random.fold_in(keys[2], 1), TOKENS // TOK_DEV)
    routes_turns = jax.random.permutation(jax.random.fold_in(keys[2], 3), TOKENS // TOK_DEV)
    routes = jax.vmap(lambda own, number: routed_block(jax.random.fold_in(keys[2], 2), own, number, TOK_DEV, N_SP // 2, 2, CAP, 1))(routes_keys, routes_turns).reshape((TOKENS, 2))
    route_weights = jnp.clip(0.25 + 0.75 * jax.random.uniform(keys[3], (TOKENS, 2), jnp.float32) ** block_levels(keys[3], (TOKENS, 2), ((0, 8),), -0.2, 0.2), 0.25, 1.0)
    gate_weight = scatter_about(keys[4], (N_SP, D, HALF), D ** -0.5, 0.125, ((0, 8), (2, 4)))
    up_weight = scatter_about(keys[5], (N_SP, D, HALF), D ** -0.5, 0.125, ((0, 8), (2, 4)))
    down_weight = scatter_about(keys[6], (N_SP, HALF, D), HID ** -0.5, 0.09375, ((0, 8), (1, 4)))
    outer_gate = scatter_about(keys[7], (TOKENS, CONV), 1.0, 6.0, ((0, 8), (1, 4)))
    inner_gate = scatter_about(keys[8], (TOKENS, CONV), 1.0, 6.0, ((0, 8), (1, 4)))
    conv_input = scatter_about(keys[9], (TOKENS, CONV), 1.0, 6.0, ((0, 8), (1, 4)))
    conv_taps = jnp.clip(jax.random.uniform(keys[10], (3, CONV), jnp.float32, -1.0, 1.0) * block_levels(keys[10], (3, CONV), ((1, 4),), -0.4, 0.0), -1.0, 1.0).astype(jnp.bfloat16)
    out_weight = scatter_about(keys[11], (D, CONV), CONV ** -0.5, 0.1875, ((1, 4),))
    return {"cotangent": cotangent, "stream": stream, "routes": routes, "route_weights": route_weights, "gate_weight": gate_weight, "up_weight": up_weight, "down_weight": down_weight, "outer_gate": outer_gate, "inner_gate": inner_gate, "conv_input": conv_input, "conv_taps": conv_taps, "out_weight": out_weight}


def reference(cotangent, stream, routes, route_weights, gate_weight, up_weight, down_weight, outer_gate, inner_gate, conv_input, conv_taps, out_weight):
    tok_count = stream.shape[0]
    model_width = stream.shape[1]
    experts = N_SP // 2
    limit = N_SP * CAP
    blocks = N_TP
    block_units = HALF // N_TP
    flat_routes = routes.reshape(-1).astype(jnp.int32)
    flat_weights = route_weights.reshape(-1).astype(jnp.float32)
    flat_tokens = (jnp.arange(2 * tok_count) // 2).astype(jnp.int32)

    def one_expert(moe_sum, index):
        hits = flat_routes == index
        picked = jnp.nonzero(hits, size=limit, fill_value=0)[0].astype(jnp.int32)
        live_mask = jnp.arange(limit) < jnp.sum(hits.astype(jnp.int32))
        tok_index = flat_tokens[picked]
        weights = jnp.where(live_mask, flat_weights[picked], jnp.float32(0.0))
        routed_rows = jnp.where(live_mask[:, None], stream[tok_index], jnp.zeros((), jnp.bfloat16))
        routed_cot = (weights[:, None] * cotangent[tok_index].astype(jnp.float32)).astype(jnp.bfloat16)
        gate_pair = lax.dynamic_slice_in_dim(gate_weight, 2 * index, 2, 0)
        up_pair = lax.dynamic_slice_in_dim(up_weight, 2 * index, 2, 0)
        down_pair = lax.dynamic_slice_in_dim(down_weight, 2 * index, 2, 0)
        gate_full = jnp.concatenate([gate_pair[0], gate_pair[1]], axis=1)
        up_full = jnp.concatenate([up_pair[0], up_pair[1]], axis=1)
        down_full = jnp.concatenate([down_pair[0], down_pair[1]], axis=0)
        gate_pre = jnp.dot(routed_rows, gate_full, preferred_element_type=jnp.float32)
        up_pre = jnp.dot(routed_rows, up_full, preferred_element_type=jnp.float32)
        hidden_grad = jnp.dot(routed_cot, down_full.T, preferred_element_type=jnp.float32)
        sigma = jax.nn.sigmoid(gate_pre)
        silu_gate = gate_pre * sigma
        hidden = (silu_gate * up_pre).astype(jnp.bfloat16)
        up_delta = (hidden_grad * silu_gate).astype(jnp.bfloat16)
        gate_delta = (hidden_grad * up_pre * sigma * (1.0 + gate_pre * (1.0 - sigma))).astype(jnp.bfloat16)
        gate_grad = jnp.dot(routed_rows.T, gate_delta, preferred_element_type=jnp.float32).astype(jnp.bfloat16)
        up_grad = jnp.dot(routed_rows.T, up_delta, preferred_element_type=jnp.float32).astype(jnp.bfloat16)
        down_grad = jnp.dot(hidden.T, routed_cot, preferred_element_type=jnp.float32).astype(jnp.bfloat16)
        gate_blocks = gate_delta.astype(jnp.float32).reshape(limit, 2 * blocks, block_units)
        up_blocks = up_delta.astype(jnp.float32).reshape(limit, 2 * blocks, block_units)
        gate_table = gate_full.astype(jnp.float32).reshape(model_width, 2 * blocks, block_units)
        up_table = up_full.astype(jnp.float32).reshape(model_width, 2 * blocks, block_units)
        block_part = jnp.einsum("sgh,dgh->gsd", gate_blocks, gate_table) + jnp.einsum("sgh,dgh->gsd", up_blocks, up_table)
        block_part = lax.optimization_barrier(block_part.astype(jnp.bfloat16)).astype(jnp.float32)
        half_sums = jnp.sum(block_part.reshape(2, blocks, limit, model_width), axis=1)
        half_sums = lax.optimization_barrier(half_sums.astype(jnp.bfloat16)).astype(jnp.float32)
        route_sum = jnp.where(live_mask[:, None], half_sums[0] + half_sums[1], jnp.float32(0.0))
        moe_sum = moe_sum.at[tok_index].add(route_sum)
        gate_out = jnp.transpose(gate_grad.reshape(model_width, 2, HALF), (1, 0, 2))
        up_out = jnp.transpose(up_grad.reshape(model_width, 2, HALF), (1, 0, 2))
        down_out = down_grad.reshape(2, HALF, model_width)
        return moe_sum, (gate_out, up_out, down_out)

    moe_sum, stacked = lax.scan(one_expert, jnp.zeros((tok_count, model_width), jnp.float32), jnp.arange(experts, dtype=jnp.int32))
    gate_grad = stacked[0].reshape(N_SP, model_width, HALF)
    up_grad = stacked[1].reshape(N_SP, model_width, HALF)
    down_grad = stacked[2].reshape(N_SP, HALF, model_width)
    moe_grad = moe_sum.astype(jnp.bfloat16)
    stream_grad = (cotangent.astype(jnp.float32) + moe_grad.astype(jnp.float32)).astype(jnp.bfloat16)

    taps = conv_taps.astype(jnp.float32)
    mixed = inner_gate.astype(jnp.float32) * conv_input.astype(jnp.float32)
    padded = jnp.pad(mixed, ((2, 0), (0, 0)))
    conv_sum = taps[0] * padded[:-2] + taps[1] * padded[1:-1] + taps[2] * padded[2:]
    conv_out = (outer_gate.astype(jnp.float32) * conv_sum).astype(jnp.bfloat16)
    out_grad = jnp.dot(stream_grad.T, conv_out, preferred_element_type=jnp.float32)
    conv_grad = jnp.dot(stream_grad, out_weight, preferred_element_type=jnp.float32)
    outer_grad = (conv_grad * conv_sum).astype(jnp.bfloat16)
    scaled = conv_grad * outer_gate.astype(jnp.float32)
    later = jnp.pad(scaled, ((0, 2), (0, 0)))
    mixed_grad = taps[2] * later[:-2] + taps[1] * later[1:-1] + taps[0] * later[2:]
    inner_grad = (mixed_grad * conv_input.astype(jnp.float32)).astype(jnp.bfloat16)
    input_grad = (mixed_grad * inner_gate.astype(jnp.float32)).astype(jnp.bfloat16)
    return (gate_grad, up_grad, down_grad, out_grad, outer_grad, inner_grad, input_grad)
```

```python
import functools

import jax
import jax.numpy as jnp
from jax import lax
from jax.experimental import pallas as pl
from jax.experimental.pallas import tpu as pltpu
from jax.sharding import PartitionSpec as P


def from_behind(block, axis, distance):
    devices = range(lax.axis_size(axis))
    route = [(i - distance, i) for i in devices if i - distance in devices]
    return lax.ppermute(block, axis, route)


def remote(src, dst, sent, landed, device):
    return pltpu.make_async_remote_copy(
        src_ref=src,
        dst_ref=dst,
        send_sem=sent,
        recv_sem=landed,
        device_id=device,
        device_id_type=pl.DeviceIdType.MESH,
    )


class Seat:
    def __init__(self, experts):
        self.sp = lax.axis_index("sp")
        self.tp = lax.axis_index("tp")
        self.x = lax.rem(self.sp, 2)
        self.z = self.sp // 2
        self.c = lax.rem(self.tp, 2)
        self.y = self.tp // 2
        self.experts = experts

    def plane(self, k):
        number, weight = 0, 1
        while weight < self.experts:
            bit = lax.rem(self.z // weight, 2)
            number = number + weight * (1 - bit if k // weight % 2 else bit)
            weight *= 2
        return number

    def over_z(self, k, swap=0):
        return (self.plane(k) * 2 + (1 - self.x if swap else self.x), self.tp)

    def over_x(self):
        return (self.z * 2 + 1 - self.x, self.tp)

    def over_y(self):
        return (self.sp, (1 - self.y) * 2 + self.c)

    def other_core(self):
        return (self.sp, self.y * 2 + 1 - self.c)

    def next_tokens(self, distance):
        groups = 2 * self.experts
        return (lax.rem(self.sp + groups + distance, groups), self.tp)


SEMS = {
    "z": lambda n: (2, n), "x": lambda n: (2, n), "y": lambda n: (2, n), "d": lambda n: (2, n, 2),
    "c": lambda n: (2, n, 4), "r1": lambda n: (n, 2), "r2": lambda n: (n, 2),
    "r3": lambda n: (n, 2), "r4": lambda n: (n,), "ag": lambda n: (3,), "g": lambda n: (n, 2),
    "gc": lambda n: (n, 2), "cz": lambda n: (n,), "cx": lambda n: (n,), "h": lambda n: (2,),
}

FIRST = (((0,), (0,)), ((), ()))
LAST = (((1,), (1,)), ((), ()))


def fused_kernel(experts, capacity, *refs):
    refs = list(refs)

    def take(count):
        got = refs[:count]
        del refs[:count]
        return got

    (routes_hbm, weights_hbm, stream_hbm, given_hbm, gate_hbm, up_hbm, down_hbm, outer_hbm,
     inner_hbm, input_hbm, taps_hbm, ow_hbm) = take(12)
    (gate_grad, up_grad, down_grad, out_grad, outer_grad, inner_grad, input_grad) = take(7)
    (routes_ref, weights_ref, block, sel, slot_weight, gate, up, down, outer, inner, given, taps, ow,
     send, rows, cots, gp_ref, up_ref, hid, delta, part, mine_part, a_ref, acc, b1a, b1b, acc2a,
     acc2b, b2a, b2b, fin, ret, sg, g_ref, c_ref, sum_ref, tail_ref, early, ext,
     late) = take(40)
    load_sem, keep_sem = take(2)
    sem = {}
    for name in SEMS:
        sem[name] = take(2)
    seat = Seat(experts)
    n_k = experts
    tokens, model = block.shape[1:]
    width = send.shape[3]
    units = gate.shape[1]
    cut = capacity // 2 // 16 * 16
    places = (rows, cots)
    slots = 2 * capacity
    f32, bf16 = jnp.float32, jnp.bfloat16
    started = []

    barrier = pltpu.get_barrier_semaphore()
    peers = [seat.over_z(k, s) for k in range(n_k) for s in range(2) if k or s]
    peers += [seat.over_y(), seat.other_core()]

    pairs = (
        (routes_hbm, routes_ref), (weights_hbm, weights_ref), (stream_hbm, block.at[0]),
        (given_hbm, block.at[1]), (inner_hbm, inner), (input_hbm, given), (gate_hbm, gate),
        (up_hbm, up), (down_hbm, down), (outer_hbm, outer), (taps_hbm, taps), (ow_hbm, ow),
    )
    loads = [pltpu.make_async_copy(s, d, load_sem.at[n]) for n, (s, d) in enumerate(pairs)]
    for load in loads:
        load.start()
    for peer in peers:
        pl.semaphore_signal(barrier, inc=1, device_id=peer, device_id_type=pl.DeviceIdType.MESH)

    def push(src, dst, name, at, device):
        sent, got = sem[name]
        copy = remote(src, dst, sent.at[at], got.at[at], device)
        copy.start()
        started.append(copy)

    def landed(spot, name, at):
        sent, got = sem[name]
        remote(spot, spot, sent.at[at], got.at[at], seat.other_core()).wait_recv()

    def cols(tp):
        return pl.ds(pl.multiple_of(tp * width, width), width)

    def total(*terms):
        value = terms[0].astype(f32)
        for term in terms[1:]:
            value = value + term.astype(f32)
        return value.astype(bf16)

    my_cols = cols(seat.tp)
    y_cols = cols((1 - seat.y) * 2 + seat.c)
    core_cols = [cols(seat.y * 2 + 1 - seat.c), cols((1 - seat.y) * 2 + 1 - seat.c)]

    tail_rows = tail_ref.shape[0]
    edge = slice(tokens - tail_rows, tokens)

    def send_halo():
        loads[4].wait()
        loads[5].wait()
        tail_ref[...] = inner[edge, :].astype(f32) * given[edge, :].astype(f32)
        pl.semaphore_wait(barrier, len(peers))
        push(tail_ref, early, "h", 0, seat.next_tokens(1))

    loads[0].wait()
    loads[1].wait()
    place_of = lax.broadcasted_iota(jnp.int32, (n_k, tokens), 0)
    number = jnp.zeros((n_k, tokens), jnp.int32)
    for k in range(n_k):
        number = jnp.where(place_of == k, seat.plane(k), number)
    named = [routes_ref[j:j + 1, :] == number for j in range(2)]
    member = jnp.where(named[0] | named[1], 1.0, 0.0)
    share = jnp.where(named[0], weights_ref[0:1, :], 0.0) + jnp.where(
        named[1], weights_ref[1:2, :], 0.0
    )
    sooner = lax.broadcasted_iota(jnp.int32, (tokens, tokens), 0) < lax.broadcasted_iota(
        jnp.int32, (tokens, tokens), 1
    )
    rank = jnp.dot(
        member.astype(bf16), jnp.where(sooner, 1.0, 0.0).astype(bf16), preferred_element_type=f32
    )
    slot = lax.broadcasted_iota(jnp.int32, (capacity, tokens), 0).astype(f32)
    for k in range(n_k):
        chosen = jnp.where(slot == rank[k:k + 1], member[k:k + 1], 0.0)
        slot_weight[k] = jnp.sum(chosen * share[k:k + 1], axis=1, keepdims=True)
        sel[k * capacity:(k + 1) * capacity, :] = chosen.astype(bf16)

    def pick(kind, k, span):
        got = jnp.dot(
            sel[k * capacity:(k + 1) * capacity, :], block[kind, :, span],
            preferred_element_type=f32,
        )
        if kind:
            got = got * slot_weight[k]
        return got.astype(bf16)

    order = list(range(n_k))

    def fill(k, kind):
        if k == order[1]:
            loads[2 + kind].wait()
        send[kind, k] = pick(kind, k, my_cols)
        if k == order[1] and kind == 0:
            send_halo()
        push(send.at[kind, k], places[kind].at[k, seat.x, :, my_cols], "z", (kind, k),
             seat.over_z(k))

    for k in order[1:]:
        for kind in range(2):
            fill(k, kind)

    def spot_of(item, x, span):
        kind, k = item
        return places[kind].at[k, x, :, span]

    def half_of(item, x, span, j):
        kind, k = item
        return places[kind].at[k, x, pl.ds(cut, capacity - cut) if j else pl.ds(0, cut), span]

    ox = 1 - seat.x

    def s1(item):
        kind, k = item
        if k == 0:
            for tp in range(model // width):
                span = slice(tp * width, (tp + 1) * width)
                places[kind][0, seat.x, :, span] = pick(kind, 0, span)
            spot = spot_of(item, seat.x, my_cols)
            push(spot, spot, "x", item, seat.over_x())
        else:
            spot = spot_of(item, seat.x, my_cols)
            landed(spot, "z", item)
            push(spot, spot, "x", item, seat.over_x())
            push(spot, spot, "y", item, seat.over_y())
            push(spot, spot, "c", item + (0,), seat.other_core())

    def s2(item):
        kind, k = item
        spot = spot_of(item, ox, my_cols)
        landed(spot, "x", item)
        if k == 0:
            push(spot, spot, "y", item, seat.over_y())
        else:
            part_spot = half_of(item, ox, my_cols, 0)
            push(part_spot, part_spot, "d", item + (0,), seat.over_y())
        push(spot, spot, "c", item + (1,), seat.other_core())
        if k:
            spot = spot_of(item, seat.x, y_cols)
            landed(spot, "y", item)
            part_spot = half_of(item, seat.x, y_cols, 1)
            push(part_spot, part_spot, "d", item + (1,), seat.over_x())
            push(spot, spot, "c", item + (2,), seat.other_core())

    def s3(item):
        kind, k = item
        spot = spot_of(item, ox, y_cols)
        if k == 0:
            landed(spot, "y", item)
        else:
            landed(half_of(item, ox, y_cols, 0), "d", item + (0,))
            landed(half_of(item, ox, y_cols, 1), "d", item + (1,))
        push(spot, spot, "c", item + (3,), seat.other_core())

    def s4(item):
        kind, k = item
        for j in range(4):
            if k == 0 and j % 2 == 0:
                continue
            landed(spot_of(item, ox if j % 2 else seat.x, core_cols[j // 2]), "c", item + (j,))

    tile = 256 if units % 256 == 0 else units

    def pre(k):
        lhs = rows[k].reshape(slots, model)
        for at in range(0, units, tile):
            gp_ref[:, at:at + tile] = jnp.dot(lhs, gate[:, at:at + tile], preferred_element_type=f32)
            up_ref[:, at:at + tile] = jnp.dot(lhs, up[:, at:at + tile], preferred_element_type=f32)

    def mid(k):
        lhs = cots[k].reshape(slots, model)
        for at in range(0, units, tile):
            span = slice(at, at + tile)
            grad = lax.dot_general(lhs, down[span, :], LAST, preferred_element_type=f32)
            gate_pre, up_pre = gp_ref[:, span], up_ref[:, span]
            sigma = jax.nn.sigmoid(gate_pre)
            silu = gate_pre * sigma
            hid[k, :, span] = (silu * up_pre).astype(bf16)
            delta[k, :, units + at:units + at + tile] = (grad * silu).astype(bf16)
            delta[k, :, span] = (grad * up_pre * sigma * (1.0 + gate_pre * (1.0 - sigma))).astype(bf16)

    def post(k, y, mine):
        out = mine_part if mine else part
        core = seat.c if mine else 1 - seat.c
        for at in range(0, width, tile):
            first = pl.ds(pl.multiple_of((y * 2 + core) * width + at, tile), tile)
            value = lax.dot_general(
                delta[k, :, :units], gate[first, :], LAST, preferred_element_type=f32
            )
            value = value + lax.dot_general(
                delta[k, :, units:], up[first, :], LAST, preferred_element_type=f32
            )
            out[k, y, :, :, at:at + tile] = value.astype(bf16).reshape(2, capacity, tile)
        if not mine:
            push(part.at[k, y], a_ref.at[k, y], "r1", (k, y), seat.other_core())

    def r2(k):
        for y in range(2):
            landed(a_ref.at[k, y], "r1", (k, y))
            acc[k, y] = total(mine_part[k, y], a_ref[k, y])
        push(acc.at[k, :, ox, pl.ds(0, cut), :], b1a.at[k], "r2", (k, 0), seat.over_x())
        push(acc.at[k, 1 - seat.y, :, pl.ds(cut, capacity - cut), :], b1b.at[k], "r2", (k, 1),
             seat.over_y())

    def r3(k):
        landed(b1a.at[k], "r2", (k, 0))
        for y in range(2):
            acc2a[k, y] = total(acc[k, y, seat.x, 0:cut, :], b1a[k, y])
        push(acc2a.at[k, 1 - seat.y], b2a.at[k], "r3", (k, 0), seat.over_y())
        landed(b1b.at[k], "r2", (k, 1))
        for x in range(2):
            acc2b[k, x] = total(acc[k, seat.y, x, cut:capacity, :], b1b[k, x])
        push(acc2b.at[k, ox], b2b.at[k], "r3", (k, 1), seat.over_x())

    def r4(k):
        landed(b2a.at[k], "r3", (k, 0))
        landed(b2b.at[k], "r3", (k, 1))
        out = fin.at[k] if k else ret.at[0]
        out[0:cut, :] = total(acc2a[k, seat.y], b2a[k])
        out[cut:capacity, :] = total(acc2b[k, seat.x], b2b[k])
        if k:
            push(fin.at[k], ret.at[k], "r4", (k,), seat.over_z(k))

    step = 256 if model % 256 == 0 else model
    pieces = [(0, at) for at in range(0, model, step)] + [(1, at) for at in range(0, model, 2 * step)]

    def work(count):
        for _ in range(min(count, len(pieces))):
            kind, at = pieces.pop(0)
            if kind == 0:
                lhs = rows[:, :, :, at:at + step].reshape(n_k * slots, step)
                for half in range(2):
                    out = up_grad if half else gate_grad
                    out[at:at + step, :] = lax.dot_general(
                        lhs, delta[:, :, half * units:(half + 1) * units].reshape(n_k * slots, units),
                        FIRST, preferred_element_type=f32,
                    ).astype(bf16)
            else:
                rhs = cots[:, :, :, at:at + 2 * step].reshape(n_k * slots, 2 * step)
                down_grad[:, at:at + 2 * step] = lax.dot_general(
                    hid[...].reshape(n_k * slots, units), rhs, FIRST, preferred_element_type=f32
                ).astype(bf16)

    def convolve():
        loads[10].wait()
        loads[9].wait()
        landed(early, "h", 0)
        earlier = jnp.where(seat.sp == 0, 0.0, early[tail_rows - 2:tail_rows, :])
        mixed = inner[...].astype(f32) * given[...].astype(f32)
        padded = jnp.concatenate([earlier, mixed], axis=0)
        t = taps[...].astype(f32)
        value = t[0:1] * padded[0:tokens] + t[1:2] * padded[1:tokens + 1]
        value = value + t[2:3] * mixed
        sum_ref[...] = value
        c_ref[0, 0] = (outer[...].astype(f32) * value).astype(bf16)
        for k in range(1, n_k):
            push(c_ref.at[0, 0], c_ref.at[k, 0], "cz", (k,), seat.over_z(k))
        push(c_ref.at[0, 0], c_ref.at[0, 1], "cx", (0,), seat.over_x())

    def spread():
        for k in range(1, n_k):
            landed(c_ref.at[k, 0], "cz", (k,))
            push(c_ref.at[k, 0], c_ref.at[k, 1], "cx", (k,), seat.over_x())

    items = [(kind, k) for k in order for kind in range(2)]
    last = len(items)
    near, far, deep = order[1], order[2], order[3]

    def chunk(item):
        kind, k = item
        s4(item)
        if kind == 0:
            pre(k)
        else:
            mid(k)
            post(k, 0, False)
            post(k, 1, False)
            post(k, 0, True)
            post(k, 1, True)

    for n in range(last + 3):
        if 2 <= n < last + 2:
            s2(items[n - 2])
        if 3 <= n < last + 3:
            s3(items[n - 3])
        if n < last:
            s1(items[n])
        if n == 3:
            for load in loads[6:9]:
                load.wait()
            convolve()
        if n == last - 1:
            spread()
        if n == last + 1:
            r2(0)
            r2(near)
        if n == last + 2:
            r3(0)
            r3(near)
            r2(far)
        if n >= 4:
            chunk(items[n - 4])
    r4(near)
    r3(far)
    chunk(items[-1])
    r4(0)
    r4(far)
    r2(deep)
    work(4)
    r3(deep)
    work(4)
    r4(deep)
    work(2)
    loads[11].wait()
    slice_width = g_ref.shape[3]
    share_rows = tokens // 2
    border = late.shape[0]
    ends = [(k, s) for k in order for s in range(2) if k or s]

    def gather():
        for k in range(1, n_k):
            landed(ret.at[k], "r4", (k,))
        moe = lax.dot_general(
            sel[...], ret[...].reshape(n_k * capacity, width), FIRST, preferred_element_type=f32
        )
        sg[:, my_cols] = total(block[1, :, my_cols], moe.astype(bf16))
        spot = sg.at[:, my_cols]
        push(spot, spot, "ag", 0, seat.over_y())
        push(spot, spot, "ag", 1, seat.other_core())

    def gather_y():
        spot = sg.at[:, y_cols]
        landed(spot, "ag", 0)
        push(spot, spot, "ag", 2, seat.other_core())

    def gather_rest():
        landed(sg.at[:, core_cols[0]], "ag", 1)
        landed(sg.at[:, core_cols[1]], "ag", 2)

    def piece(k, swap, core):
        d = seat.plane(k) * 2 + (ox if swap else seat.x)
        first = pl.ds(pl.multiple_of(core * share_rows, share_rows), share_rows)
        return sg.at[first, pl.ds(pl.multiple_of(d * slice_width, slice_width), slice_width)]

    def g_half(k, swap, core):
        first = pl.ds(pl.multiple_of(core * share_rows, share_rows), share_rows)
        return g_ref.at[k, swap, first, :]

    def g_send():
        for k, s in reversed(ends):
            push(piece(k, s, seat.c), g_half(k, s, seat.c), "g", (k, s), seat.over_z(k, s))

    def project():
        conv_grad = jnp.dot(sg[...], ow[...], preferred_element_type=f32)
        ext[0:tokens, :] = conv_grad * outer[...].astype(f32)
        push(ext.at[0:border, :], late, "h", 1, seat.next_tokens(-1))
        outer_grad[...] = (conv_grad * sum_ref[...]).astype(bf16)
        own = sg[:, pl.ds(pl.multiple_of(seat.sp * slice_width, slice_width), slice_width)]
        out_grad[...] = lax.dot_general(own, c_ref[0, 0], FIRST, preferred_element_type=f32)

    def finish_conv():
        landed(late, "h", 1)
        ext[tokens:tokens + border, :] = jnp.where(seat.sp == 2 * n_k - 1, 0.0, late[...])
        t = taps[...].astype(f32)
        mixed_grad = t[2:3] * ext[0:tokens, :]
        mixed_grad = mixed_grad + t[1:2] * ext[1:tokens + 1, :]
        mixed_grad = mixed_grad + t[0:1] * ext[2:tokens + 2, :]
        inner_grad[...] = (mixed_grad * given[...].astype(f32)).astype(bf16)
        input_grad[...] = (mixed_grad * inner[...].astype(f32)).astype(bf16)

    def g_wait(k, s):
        spot = g_half(k, s, seat.c)
        landed(spot, "g", (k, s))
        push(spot, spot, "gc", (k, s), seat.other_core())

    def g_add(k, s):
        landed(g_half(k, s, 1 - seat.c), "gc", (k, s))
        out_grad[...] += lax.dot_general(
            g_ref[k, s], c_ref[k, s], FIRST, preferred_element_type=f32
        )

    def drain():
        for copy in started:
            copy.wait_send()

    gather()
    work(2)
    gather_y()
    gather_rest()
    g_send()
    project()
    work(len(pieces))
    for k in range(n_k):
        landed(c_ref.at[k, 1], "cx", (k,))
    for k, s in ends[:4]:
        g_wait(k, s)
    finish_conv()
    for k, s in ends[4:]:
        g_wait(k, s)
    for k, s in ends:
        g_add(k, s)
    drain()


def write_kernel(count, *refs):
    sources, targets, done = refs[:count], refs[count:2 * count], refs[2 * count]
    copies = [pltpu.make_async_copy(sources[n], targets[n], done.at[n]) for n in range(count)]
    for copy in copies:
        copy.start()
    for copy in copies:
        copy.wait()


def in_vmem(count):
    return [pl.BlockSpec(memory_space=pltpu.VMEM)] * count


def in_hbm(count):
    return [pl.BlockSpec(memory_space=pltpu.HBM)] * count


def fused(cotangent, stream, routes, route_weights, gate, up, down, outer, inner, given, taps,
          out_weight, experts, capacity):
    tokens, model = stream.shape
    units = gate.shape[1]
    channels = outer.shape[1]
    width = model // 4
    slice_width = model // (2 * experts)
    border, tail_rows = min(8, tokens), min(16, tokens)
    cut = capacity // 2 // 16 * 16
    rest = capacity - cut
    bf16, f32 = jnp.bfloat16, jnp.float32
    n = experts
    slots = 2 * capacity
    gate_shape = jax.ShapeDtypeStruct((model, units), bf16)
    own = jax.ShapeDtypeStruct((tokens, channels), bf16)
    outs = (
        gate_shape, gate_shape, jax.ShapeDtypeStruct((units, model), bf16),
        jax.ShapeDtypeStruct((slice_width, channels), f32), own, own, own,
    )
    half = (n, 2, 2, capacity, width)
    scratch = [
        ((2, tokens), jnp.int32), ((2, tokens), f32), ((2, tokens, model), bf16),
        ((n * capacity, tokens), bf16), ((n, capacity, 1), f32),
        ((model, units), bf16), ((model, units), bf16), ((units, model), bf16),
        ((tokens, channels), bf16), ((tokens, channels), bf16), ((tokens, channels), bf16),
        ((3, channels), bf16), ((model, channels), bf16),
        ((2, n, capacity, width), bf16), ((n, 2, capacity, model), bf16),
        ((n, 2, capacity, model), bf16), ((slots, units), f32), ((slots, units), f32),
        ((n, slots, units), bf16), ((n, slots, 2 * units), bf16),
        (half, bf16), (half, bf16), (half, bf16), (half, bf16),
        ((n, 2, cut, width), bf16), ((n, 2, rest, width), bf16),
        ((n, 2, cut, width), bf16), ((n, 2, rest, width), bf16),
        ((n, cut, width), bf16), ((n, rest, width), bf16),
        ((n, capacity, width), bf16), ((n, capacity, width), bf16),
        ((tokens, model), bf16), ((n, 2, tokens, slice_width), bf16),
        ((n, 2, tokens, channels), bf16), ((tokens, channels), f32),
        ((tail_rows, channels), f32), ((tail_rows, channels), f32),
        ((tokens + border, channels), f32), ((border, channels), f32),
    ]
    sems = [pltpu.SemaphoreType.DMA((12,)), pltpu.SemaphoreType.DMA((1,))]
    for shape_of in SEMS.values():
        sems += [pltpu.SemaphoreType.DMA(shape_of(n))] * 2
    made = pl.pallas_call(
        functools.partial(fused_kernel, experts, capacity),
        out_shape=tuple(pltpu.VMEM(out.shape, out.dtype) for out in outs),
        in_specs=in_hbm(12),
        out_specs=tuple(in_vmem(7)),
        scratch_shapes=[pltpu.VMEM(*s) for s in scratch] + sems,
        compiler_params=pltpu.CompilerParams(
            collective_id=0, has_side_effects=True, vmem_limit_bytes=48 * 1024 * 1024
        ),
        name="fused",
    )(*[
        pltpu.with_memory_space_constraint(value, pltpu.HBM)
        for value in (
            routes.T, route_weights.T, stream, cotangent, gate, up, down, outer, inner, given,
            taps, out_weight,
        )
    ])
    written = pl.pallas_call(
        functools.partial(write_kernel, len(outs)),
        out_shape=outs,
        in_specs=in_vmem(len(outs)),
        out_specs=tuple(in_hbm(len(outs))),
        scratch_shapes=[pltpu.SemaphoreType.DMA((len(outs),))],
        compiler_params=pltpu.CompilerParams(vmem_limit_bytes=1024 * 1024),
        name="write",
    )(*made)
    return tuple(out[None] for out in written[:3]) + tuple(written[3:])


def per_device(
    cotangent,
    stream,
    routes,
    route_weights,
    gate_weight,
    up_weight,
    down_weight,
    outer_gate,
    inner_gate,
    conv_input,
    conv_taps,
    out_weight,
):
    groups = lax.axis_size("sp")
    tp_count = lax.axis_size("tp")
    experts = groups // 2
    tok_rows = stream.shape[0]
    model_width = stream.shape[1]
    capacity = 3 * tok_rows // experts
    slot_total = experts * capacity
    contract_first = (((0,), (0,)), ((), ()))
    contract_last = (((1,), (1,)), ((), ()))
    block_width = model_width // tp_count
    slots = groups * capacity
    even = experts & (experts - 1) == 0 and tp_count == 4
    if even and capacity % 32 == 0 and block_width % 128 == 0:
        return fused(
            cotangent, stream, routes, route_weights, gate_weight[0], up_weight[0],
            down_weight[0], outer_gate, inner_gate, conv_input, conv_taps, out_weight,
            experts, capacity,
        )
    taps = conv_taps.astype(jnp.float32)
    outer_f = outer_gate.astype(jnp.float32)
    inner_f = inner_gate.astype(jnp.float32)
    input_f = conv_input.astype(jnp.float32)
    mixed = inner_f * input_f
    flat_routes = routes.reshape(-1)
    choose = (flat_routes[:, None] == jnp.arange(experts, dtype=jnp.int32)[None, :]).astype(
        jnp.int32
    )
    before = jnp.cumsum(choose, axis=0) - choose
    slot_place = flat_routes * capacity + jnp.sum(before * choose, axis=1)
    slot_table = (jnp.arange(slot_total, dtype=jnp.int32)[:, None] == slot_place[None, :]).astype(
        jnp.float32
    )
    select = jnp.sum(slot_table.reshape(slot_total, tok_rows, 2), axis=2).astype(jnp.bfloat16)
    slot_weight = jnp.sum(slot_table * route_weights.reshape(-1)[None, :], axis=1)
    offset = lax.axis_index("tp") * block_width
    rows_part = lax.dynamic_slice_in_dim(stream, offset, block_width, 1)
    cot_part = lax.dynamic_slice_in_dim(cotangent, offset, block_width, 1)
    sent_rows = jnp.dot(select, rows_part, preferred_element_type=jnp.float32).astype(jnp.bfloat16)
    sent_cot = (
        jnp.dot(select, cot_part, preferred_element_type=jnp.float32) * slot_weight[:, None]
    ).astype(jnp.bfloat16)
    sent_rows = jnp.repeat(sent_rows.reshape(experts, capacity, -1), 2, axis=0)
    sent_cot = jnp.repeat(sent_cot.reshape(experts, capacity, -1), 2, axis=0)
    recv_rows, recv_cot = (
        lax.all_to_all(sent_rows, "sp", split_axis=0, concat_axis=0, tiled=True),
        lax.all_to_all(sent_cot, "sp", split_axis=0, concat_axis=0, tiled=True),
    )
    recv_rows, recv_cot = (
        lax.all_gather(recv_rows, "tp", axis=2, tiled=True),
        lax.all_gather(recv_cot, "tp", axis=2, tiled=True),
    )
    routed_rows = recv_rows.reshape(slots, model_width)
    routed_cot = recv_cot.reshape(slots, model_width)
    earlier = from_behind(mixed[-2:], "sp", 1)
    gate_local = gate_weight[0]
    up_local = up_weight[0]
    down_local = down_weight[0]
    gate_pre = jnp.dot(routed_rows, gate_local, preferred_element_type=jnp.float32)
    up_pre = jnp.dot(routed_rows, up_local, preferred_element_type=jnp.float32)
    hidden_grad = lax.dot_general(
        routed_cot, down_local, contract_last, preferred_element_type=jnp.float32
    )
    sigma = jax.nn.sigmoid(gate_pre)
    silu_gate = gate_pre * sigma
    hidden = (silu_gate * up_pre).astype(jnp.bfloat16)
    up_delta = (hidden_grad * silu_gate).astype(jnp.bfloat16)
    gate_delta = (hidden_grad * up_pre * sigma * (1.0 + gate_pre * (1.0 - sigma))).astype(
        jnp.bfloat16
    )
    row_partial = lax.dot_general(
        gate_delta, gate_local, contract_last, preferred_element_type=jnp.float32
    )
    row_partial = row_partial + lax.dot_general(
        up_delta, up_local, contract_last, preferred_element_type=jnp.float32
    )
    padded = jnp.concatenate([earlier, mixed], axis=0)
    conv_sum = taps[0] * padded[:-2] + taps[1] * padded[1:-1] + taps[2] * padded[2:]
    conv_out = (outer_f * conv_sum).astype(jnp.bfloat16)
    gate_grad = lax.dot_general(
        routed_rows, gate_delta, contract_first, preferred_element_type=jnp.float32
    ).astype(jnp.bfloat16)[None]
    up_grad = lax.dot_general(
        routed_rows, up_delta, contract_first, preferred_element_type=jnp.float32
    ).astype(jnp.bfloat16)[None]
    down_grad = lax.dot_general(
        hidden, routed_cot, contract_first, preferred_element_type=jnp.float32
    ).astype(jnp.bfloat16)[None]
    half_sums = lax.psum_scatter(
        row_partial.astype(jnp.bfloat16), "tp", scatter_dimension=1, tiled=True
    ).astype(jnp.float32)
    block_width = half_sums.shape[1]
    half_grad = half_sums.reshape(groups, capacity, block_width).astype(jnp.bfloat16)
    returned = lax.all_to_all(half_grad, "sp", split_axis=0, concat_axis=0, tiled=True)
    returned = returned.reshape(experts, 2, capacity, block_width)
    select_three = select.reshape(experts, capacity, tok_rows)
    moe_part = jnp.einsum(
        "ecr,emcd->rd", select_three, returned, preferred_element_type=jnp.float32
    ).astype(jnp.bfloat16)
    moe_grad = lax.all_gather(moe_part, "tp", axis=1, tiled=True)
    stream_grad = (cotangent.astype(jnp.float32) + moe_grad.astype(jnp.float32)).astype(
        jnp.bfloat16
    )
    out_grad = lax.psum_scatter(
        lax.dot_general(
            stream_grad, conv_out, contract_first, preferred_element_type=jnp.float32
        ).astype(jnp.bfloat16),
        "sp",
        scatter_dimension=0,
        tiled=True,
    ).astype(jnp.float32)
    conv_grad = jnp.dot(stream_grad, out_weight, preferred_element_type=jnp.float32)
    outer_grad = (conv_grad * conv_sum).astype(jnp.bfloat16)
    scaled = conv_grad * outer_f
    later = from_behind(scaled[:2], "sp", -1)
    extended = jnp.concatenate([scaled, later], axis=0)
    mixed_grad = taps[2] * extended[:-2] + taps[1] * extended[1:-1] + taps[0] * extended[2:]
    inner_grad = (mixed_grad * input_f).astype(jnp.bfloat16)
    input_grad = (mixed_grad * inner_f).astype(jnp.bfloat16)
    return (gate_grad, up_grad, down_grad, out_grad, outer_grad, inner_grad, input_grad)


def solution(mesh):
    placed = (
        P("sp", None),
        P("sp", None),
        P("sp", None),
        P("sp", None),
        P("sp", None, "tp"),
        P("sp", None, "tp"),
        P("sp", "tp", None),
        P("sp", "tp"),
        P("sp", "tp"),
        P("sp", "tp"),
        P(None, "tp"),
        P(None, "tp"),
    )
    return jax.shard_map(
        per_device,
        mesh=mesh,
        in_specs=placed,
        out_specs=(
            P("sp", None, "tp"),
            P("sp", None, "tp"),
            P("sp", "tp", None),
            P("sp", "tp"),
            P("sp", "tp"),
            P("sp", "tp"),
            P("sp", "tp"),
        ),
        check_vma=False,
    )
```

```python
import functools

import jax
import jax.numpy as jnp
from jax import lax
from jax.experimental import pallas as pl
from jax.experimental.pallas import tpu as pltpu
from jax.sharding import PartitionSpec as P


def from_behind(block, axis, distance):
    devices = range(lax.axis_size(axis))
    route = [(i - distance, i) for i in devices if i - distance in devices]
    return lax.ppermute(block, axis, route)


def remote(src, dst, sent, landed, device):
    return pltpu.make_async_remote_copy(
        src_ref=src,
        dst_ref=dst,
        send_sem=sent,
        recv_sem=landed,
        device_id=device,
        device_id_type=pl.DeviceIdType.MESH,
    )


class Seat:
    def __init__(self, experts):
        self.sp = lax.axis_index("sp")
        self.tp = lax.axis_index("tp")
        self.x = lax.rem(self.sp, 2)
        self.z = self.sp // 2
        self.c = lax.rem(self.tp, 2)
        self.y = self.tp // 2
        self.experts = experts

    def plane(self, k):
        number, weight = 0, 1
        while weight < self.experts:
            bit = lax.rem(self.z // weight, 2)
            number = number + weight * (1 - bit if k // weight % 2 else bit)
            weight *= 2
        return number

    def between(self, plane):
        number, weight = 0, 1
        while weight < self.experts:
            number = number + weight * lax.rem(self.z // weight + plane // weight, 2)
            weight *= 2
        return number

    def over_z(self, k, swap=0):
        return (self.plane(k) * 2 + (1 - self.x if swap else self.x), self.tp)

    def over_x(self):
        return (self.z * 2 + 1 - self.x, self.tp)

    def over_y(self):
        return (self.sp, (1 - self.y) * 2 + self.c)

    def other_core(self):
        return (self.sp, self.y * 2 + 1 - self.c)

    def next_tokens(self, distance):
        groups = 2 * self.experts
        return (lax.rem(self.sp + groups + distance, groups), self.tp)


SEMS = {
    "z": lambda n: (2, n), "x": lambda n: (2, n), "y": lambda n: (2, n), "d": lambda n: (2, n),
    "c0": lambda n: (2,), "c": lambda n: (2, n), "r1": lambda n: (n,), "r2": lambda n: (n, 2),
    "r3": lambda n: (n, 2), "r4": lambda n: (1,), "ag": lambda n: (3,), "g": lambda n: (n, 2),
    "gc": lambda n: (1,), "cz": lambda n: (1,), "cx": lambda n: (1,), "h0": lambda n: (1,),
    "h1": lambda n: (1,),
}

FIRST = (((0,), (0,)), ((), ()))
LAST = (((1,), (1,)), ((), ()))


def fused_kernel(experts, capacity, *refs):
    refs = list(refs)

    def take(count):
        got = refs[:count]
        del refs[:count]
        return got

    (routes_hbm, weights_hbm, stream_hbm, given_hbm, gate_hbm, up_hbm, down_hbm, outer_hbm,
     inner_hbm, input_hbm, taps_hbm, ow_hbm) = take(12)
    (gate_grad, up_grad, down_grad, out_grad, outer_grad, inner_grad, input_grad) = take(7)
    (routes_ref, weights_ref, block, sel, slot_weight, gate, up, down, outer, inner, given, taps, ow,
     send, rows, cots, gp_ref, up_ref, hid, delta, part, mine_part, a_ref, acc, b1a, b1b, acc2a,
     acc2b, b2a, b2b, fin, ret, sg, g_ref, c_ref, sum_ref, tail_ref, early, ext,
     late) = take(40)
    load_sem, sent_sem = take(2)
    names = list(SEMS)
    sem = dict(zip(names, take(len(names))))
    seat = Seat(experts)
    n_k = experts
    tokens, model = block.shape[1:]
    width = send.shape[3]
    units = gate.shape[1]
    cut = capacity // 2 // 16 * 16
    places = (rows, cots)
    slots = 2 * capacity
    f32, bf16 = jnp.float32, jnp.bfloat16

    barrier = pltpu.get_barrier_semaphore()
    peers = [seat.over_z(k, s) for k in range(n_k) for s in range(2) if k or s]
    peers += [seat.over_y(), seat.other_core()]

    pairs = (
        (routes_hbm, routes_ref), (weights_hbm, weights_ref), (stream_hbm, block.at[0]),
        (given_hbm, block.at[1]), (inner_hbm, inner), (input_hbm, given), (gate_hbm, gate),
        (up_hbm, up), (down_hbm, down), (outer_hbm, outer), (taps_hbm, taps), (ow_hbm, ow),
    )
    loads = [pltpu.make_async_copy(s, d, load_sem.at[n]) for n, (s, d) in enumerate(pairs)]
    for load in loads:
        load.start()
    for peer in peers:
        pl.semaphore_signal(barrier, inc=1, device_id=peer, device_id_type=pl.DeviceIdType.MESH)

    def push(src, dst, name, at, device):
        remote(src, dst, sent_sem.at[names.index(name)], sem[name].at[at], device).start()

    def landed(spot, name, at):
        remote(spot, spot, sent_sem.at[0], sem[name].at[at], seat.other_core()).wait_recv()

    def cols(tp):
        return pl.ds(pl.multiple_of(tp * width, width), width)

    def total(*terms):
        value = terms[0].astype(f32)
        for term in terms[1:]:
            value = value + term.astype(f32)
        return value.astype(bf16)

    my_cols = cols(seat.tp)
    y_cols = cols((1 - seat.y) * 2 + seat.c)
    core_cols = [cols(seat.y * 2 + 1 - seat.c), cols((1 - seat.y) * 2 + 1 - seat.c)]

    tail_rows = tail_ref.shape[0]
    edge = slice(tokens - tail_rows, tokens)

    def send_halo():
        loads[4].wait()
        loads[5].wait()
        tail_ref[...] = inner[edge, :].astype(f32) * given[edge, :].astype(f32)
        pl.semaphore_wait(barrier, len(peers))
        push(tail_ref, early, "h0", 0, seat.next_tokens(1))

    loads[0].wait()
    loads[1].wait()
    place_of = lax.broadcasted_iota(jnp.int32, (n_k, tokens), 0)
    number = jnp.zeros((n_k, tokens), jnp.int32)
    for k in range(n_k):
        number = jnp.where(place_of == k, seat.plane(k), number)
    named = [routes_ref[j:j + 1, :] == number for j in range(2)]
    member = jnp.where(named[0] | named[1], 1.0, 0.0)
    share = jnp.where(named[0], weights_ref[0:1, :], 0.0) + jnp.where(
        named[1], weights_ref[1:2, :], 0.0
    )
    sooner = lax.broadcasted_iota(jnp.int32, (tokens, tokens), 0) < lax.broadcasted_iota(
        jnp.int32, (tokens, tokens), 1
    )
    rank = jnp.dot(
        member.astype(bf16), jnp.where(sooner, 1.0, 0.0).astype(bf16), preferred_element_type=f32
    )
    slot = lax.broadcasted_iota(jnp.int32, (capacity, tokens), 0).astype(f32)
    for k in range(n_k):
        chosen = jnp.where(slot == rank[k:k + 1], member[k:k + 1], 0.0)
        slot_weight[k] = jnp.sum(chosen * share[k:k + 1], axis=1, keepdims=True)
        sel[k * capacity:(k + 1) * capacity, :] = chosen.astype(bf16)

    def pick(kind, k, span):
        got = jnp.dot(
            sel[k * capacity:(k + 1) * capacity, :], block[kind, :, span],
            preferred_element_type=f32,
        )
        if kind:
            got = got * slot_weight[k]
        return got.astype(bf16)

    order = [0] + [k for k in range(1, n_k) if k != 2] + [2]

    def fill(k, kind):
        send[kind, k] = pick(kind, k, my_cols)

    def launch(k, kind):
        push(send.at[kind, k], places[kind].at[k, seat.x, :, my_cols], "z", (kind, k),
             seat.over_z(k))

    def fill_own(kind):
        for tp in range(model // width):
            span = slice(tp * width, (tp + 1) * width)
            places[kind][0, seat.x, :, span] = pick(kind, 0, span)

    def spot_of(item, x, span):
        kind, k = item
        return places[kind].at[k, x, :, span]

    def half_of(item, x, span, j):
        kind, k = item
        return places[kind].at[k, x, pl.ds(cut, capacity - cut) if j else pl.ds(0, cut), span]

    ox = 1 - seat.x

    def to_core(spot, item):
        kind, k = item
        push(spot, spot, "c" if k else "c0", item if k else kind, seat.other_core())

    def s1(item):
        kind, k = item
        if k == 0:
            spot = spot_of(item, seat.x, my_cols)
            push(spot, spot, "x", item, seat.over_x())
        else:
            spot = spot_of(item, seat.x, my_cols)
            landed(spot, "z", item)
            push(spot, spot, "x", item, seat.over_x())
            push(spot, spot, "y", item, seat.over_y())
            push(spot, spot, "c", item, seat.other_core())

    def s2(item):
        kind, k = item
        spot = spot_of(item, ox, my_cols)
        landed(spot, "x", item)
        if k == 0:
            push(spot, spot, "y", item, seat.over_y())
        else:
            part_spot = half_of(item, ox, my_cols, 0)
            push(part_spot, part_spot, "d", item, seat.over_y())
        to_core(spot, item)
        if k:
            spot = spot_of(item, seat.x, y_cols)
            landed(spot, "y", item)
            part_spot = half_of(item, seat.x, y_cols, 1)
            push(part_spot, part_spot, "d", item, seat.over_x())
            push(spot, spot, "c", item, seat.other_core())

    def s3(item):
        kind, k = item
        spot = spot_of(item, ox, y_cols)
        if k == 0:
            landed(spot, "y", item)
        else:
            landed(spot, "d", item)
        to_core(spot, item)

    def s4(item):
        kind, k = item
        if k == 0:
            landed(rows.at[0, :, :, 0:width], "c0", kind)
        else:
            landed(rows.at[k, :, :, 0:2 * width], "c", item)

    tile = 256 if units % 256 == 0 else units

    def pre(k):
        lhs = rows[k].reshape(slots, model)
        for at in range(0, units, tile):
            gp_ref[:, at:at + tile] = jnp.dot(lhs, gate[:, at:at + tile], preferred_element_type=f32)
            up_ref[:, at:at + tile] = jnp.dot(lhs, up[:, at:at + tile], preferred_element_type=f32)

    def mid(k):
        lhs = cots[k].reshape(slots, model)
        for at in range(0, units, tile):
            span = slice(at, at + tile)
            grad = lax.dot_general(lhs, down[span, :], LAST, preferred_element_type=f32)
            gate_pre, up_pre = gp_ref[:, span], up_ref[:, span]
            sigma = jax.nn.sigmoid(gate_pre)
            silu = gate_pre * sigma
            hid[k, :, span] = (silu * up_pre).astype(bf16)
            delta[k, :, units + at:units + at + tile] = (grad * silu).astype(bf16)
            delta[k, :, span] = (grad * up_pre * sigma * (1.0 + gate_pre * (1.0 - sigma))).astype(bf16)

    def post(k, y, mine):
        out = mine_part if mine else part
        core = seat.c if mine else 1 - seat.c
        for at in range(0, width, tile):
            first = pl.ds(pl.multiple_of((y * 2 + core) * width + at, tile), tile)
            value = lax.dot_general(
                delta[k, :, :units], gate[first, :], LAST, preferred_element_type=f32
            )
            value = value + lax.dot_general(
                delta[k, :, units:], up[first, :], LAST, preferred_element_type=f32
            )
            out[k, y, :, :, at:at + tile] = value.astype(bf16).reshape(2, capacity, tile)
        if not mine:
            push(part.at[k, y], a_ref.at[k, y], "r1", k, seat.other_core())

    def r2(k):
        landed(a_ref.at[k], "r1", k)
        for y in range(2):
            acc[k, y] = total(mine_part[k, y], a_ref[k, y])
        push(acc.at[k, :, ox, pl.ds(0, cut), :], b1a.at[k], "r2", (k, 0), seat.over_x())
        push(acc.at[k, 1 - seat.y, :, pl.ds(cut, capacity - cut), :], b1b.at[k], "r2", (k, 1),
             seat.over_y())

    def r3(k):
        landed(b1a.at[k], "r2", (k, 0))
        for y in range(2):
            acc2a[k, y] = total(acc[k, y, seat.x, 0:cut, :], b1a[k, y])
        push(acc2a.at[k, 1 - seat.y], b2a.at[k], "r3", (k, 0), seat.over_y())
        landed(b1b.at[k], "r2", (k, 1))
        for x in range(2):
            acc2b[k, x] = total(acc[k, seat.y, x, cut:capacity, :], b1b[k, x])
        push(acc2b.at[k, ox], b2b.at[k], "r3", (k, 1), seat.over_x())

    def r4(k):
        landed(b2a.at[k], "r3", (k, 0))
        landed(b2b.at[k], "r3", (k, 1))
        out = fin.at[k] if k else ret.at[0]
        out[0:cut, :] = total(acc2a[k, seat.y], b2a[k])
        out[cut:capacity, :] = total(acc2b[k, seat.x], b2b[k])
        if k:
            push(fin.at[k], ret.at[k], "r4", 0, seat.over_z(k))

    step = 256 if model % 256 == 0 else model
    pieces = [(0, at) for at in range(0, model, step)] + [(1, at) for at in range(0, model, 2 * step)]

    def work(count):
        for _ in range(min(count, len(pieces))):
            kind, at = pieces.pop(0)
            if kind == 0:
                lhs = rows[:, :, :, at:at + step].reshape(n_k * slots, step)
                for half in range(2):
                    out = up_grad if half else gate_grad
                    out[at:at + step, :] = lax.dot_general(
                        lhs, delta[:, :, half * units:(half + 1) * units].reshape(n_k * slots, units),
                        FIRST, preferred_element_type=f32,
                    ).astype(bf16)
            else:
                rhs = cots[:, :, :, at:at + 2 * step].reshape(n_k * slots, 2 * step)
                down_grad[:, at:at + 2 * step] = lax.dot_general(
                    hid[...].reshape(n_k * slots, units), rhs, FIRST, preferred_element_type=f32
                ).astype(bf16)

    share_rows = tokens // 2
    slice_width = g_ref.shape[4]

    def convolve():
        loads[10].wait()
        loads[9].wait()
        landed(early, "h0", 0)
        earlier = jnp.where(seat.sp == 0, 0.0, early[tail_rows - 2:tail_rows, :])
        mixed = inner[...].astype(f32) * given[...].astype(f32)
        padded = jnp.concatenate([earlier, mixed], axis=0)
        t = taps[...].astype(f32)
        value = t[0:1] * padded[0:tokens] + t[1:2] * padded[1:tokens + 1]
        value = value + t[2:3] * mixed
        sum_ref[...] = value
        value = (outer[...].astype(f32) * value).astype(bf16)
        for j in range(2):
            c_ref[j, 0, 0] = value[j * share_rows:(j + 1) * share_rows]

    def spread_z():
        for k in range(1, n_k):
            push(c_ref.at[:, 0, 0], c_ref.at[:, k, 0], "cz", 0, seat.over_z(k))

    def spread_x():
        landed(c_ref.at[:, 1:n_k, 0], "cz", 0)
        for k in range(n_k):
            push(c_ref.at[:, k, 0], c_ref.at[:, k, 1], "cx", 0, seat.over_x())

    items = [(kind, k) for k in order for kind in range(2)]
    last = len(items)
    near, far, deep = order[1], order[2], order[3]

    def experts_of(k):
        mid(k)
        post(k, 0, False)
        post(k, 1, False)
        post(k, 0, True)
        post(k, 1, True)

    loads[2].wait()
    fill(near, 0)
    fill_own(0)
    send_halo()
    s1(items[0])
    launch(near, 0)
    loads[3].wait()
    fill(near, 1)
    launch(near, 1)
    fill_own(1)
    s1(items[1])
    for k in order[2:]:
        for kind in range(2):
            fill(k, kind)
            launch(k, kind)
    s2(items[0])
    s1(items[2])
    s2(items[1])
    s3(items[0])
    s1(items[3])
    for load in loads[6:9]:
        load.wait()
    convolve()
    s2(items[2])
    s3(items[1])
    s1(items[4])
    s4(items[0])
    pre(0)
    s2(items[3])
    s3(items[2])
    s1(items[5])
    s4(items[1])
    experts_of(0)
    s2(items[4])
    s3(items[3])
    s1(items[6])
    s4(items[2])
    pre(near)
    s2(items[5])
    s3(items[4])
    s1(items[7])
    spread_z()
    s4(items[3])
    experts_of(near)
    s2(items[6])
    s3(items[5])
    s4(items[4])
    pre(far)
    s2(items[7])
    r2(0)
    r2(near)
    s4(items[5])
    experts_of(far)
    s3(items[6])
    s3(items[7])
    r2(far)
    s4(items[6])
    pre(deep)
    r3(0)
    r3(near)
    s4(items[7])
    mid(deep)
    post(deep, 0, False)
    post(deep, 1, False)
    r3(far)
    post(deep, 0, True)
    post(deep, 1, True)
    r4(near)
    r2(deep)
    r4(0)
    r4(far)
    work(6)
    r3(deep)
    spread_x()
    work(4)
    r4(deep)
    work(2)
    loads[11].wait()
    border = late.shape[0]
    ends = [(k, s) for k in order for s in range(2) if k or s]

    def gather():
        landed(ret.at[1:n_k], "r4", 0)
        moe = lax.dot_general(
            sel[...], ret[...].reshape(n_k * capacity, width), FIRST, preferred_element_type=f32
        )
        sg[:, my_cols] = total(block[1, :, my_cols], moe.astype(bf16))
        spot = sg.at[:, my_cols]
        push(spot, spot, "ag", 0, seat.over_y())
        push(spot, spot, "ag", 1, seat.other_core())

    def flip(bits):
        number, weight = 0, 1
        while weight < n_k:
            number = number + weight * lax.rem(bits // weight + seat.tp // weight, 2)
            weight *= 2
        return number

    def g_half(k, swap, core):
        return g_ref.at[core, k, swap]

    mine_half = pl.ds(pl.multiple_of(seat.c * share_rows, share_rows), share_rows)

    def g_send(j):
        plane = flip(j)
        k = seat.between(plane)
        for s in range(2):
            d = plane * 2 + (ox if s else seat.x)
            src = sg.at[mine_half, pl.ds(pl.multiple_of(d * slice_width, slice_width), slice_width)]
            if s:
                push(src, g_half(k, s, seat.c), "g", (k, s), (d, seat.tp))
            else:
                @pl.when(k > 0)
                def _():
                    push(src, g_half(k, s, seat.c), "g", (k, s), (d, seat.tp))

    def gather_core():
        landed(sg.at[:, core_cols[0]], "ag", 1)

    def gather_y():
        spot = sg.at[:, y_cols]
        landed(spot, "ag", 0)
        push(spot, spot, "ag", 2, seat.other_core())

    def gather_rest():
        landed(sg.at[:, core_cols[1]], "ag", 2)

    def project():
        conv_grad = jnp.dot(sg[...], ow[...], preferred_element_type=f32)
        ext[0:tokens, :] = conv_grad * outer[...].astype(f32)
        push(ext.at[0:border, :], late, "h1", 0, seat.next_tokens(-1))
        outer_grad[...] = (conv_grad * sum_ref[...]).astype(bf16)
        own = pl.ds(pl.multiple_of(seat.sp * slice_width, slice_width), slice_width)
        for j in range(2):
            g_ref[j, 0, 0] = sg[j * share_rows:(j + 1) * share_rows, own]

    def finish_conv():
        landed(late, "h1", 0)
        ext[tokens:tokens + border, :] = jnp.where(seat.sp == 2 * n_k - 1, 0.0, late[...])
        t = taps[...].astype(f32)
        mixed_grad = t[2:3] * ext[0:tokens, :]
        mixed_grad = mixed_grad + t[1:2] * ext[1:tokens + 1, :]
        mixed_grad = mixed_grad + t[0:1] * ext[2:tokens + 2, :]
        inner_grad[...] = (mixed_grad * given[...].astype(f32)).astype(bf16)
        input_grad[...] = (mixed_grad * inner[...].astype(f32)).astype(bf16)

    def g_wait(k, s):
        spot = g_half(k, s, seat.c)
        landed(spot, "g", (k, s))
        push(spot, spot, "gc", 0, seat.other_core())

    def g_add(core):
        rows_of = 2 * n_k * share_rows
        return lax.dot_general(
            g_ref[core].reshape(rows_of, slice_width), c_ref[core].reshape(rows_of, -1), FIRST,
            preferred_element_type=f32,
        )

    def g_own():
        landed(c_ref.at[:, :, 1], "cx", 0)
        out_grad[...] = g_add(seat.c)

    def g_other():
        landed(sg.at[0:share_rows, 0:len(ends) * slice_width], "gc", 0)
        out_grad[...] += g_add(1 - seat.c)

    def drain():
        pieces_sent = sg.at[0:share_rows, 0:len(ends) * slice_width]
        spans = {
            "z": send.at[:, 1:n_k], "x": rows.at[:, :, :, 0:width], "y": rows.at[:, :, :, 0:width],
            "d": send.at[:, 1:n_k], "c0": rows.at[0:2, :, :, 0:width], "c": rows.at[0:n_k - 1],
            "r1": part, "r2": part.at[:, 0], "r3": part.at[:, 0, 0], "r4": part.at[0:n_k - 1, 0, 0],
            "ag": sg.at[:, 0:3 * width], "g": pieces_sent, "gc": pieces_sent,
            "cz": c_ref.at[:, 1:n_k, 0], "cx": c_ref.at[:, :, 0], "h0": tail_ref,
            "h1": ext.at[0:border, :],
        }
        for n, name in enumerate(names):
            span = spans[name]
            remote(span, span, sent_sem.at[n], load_sem.at[0], seat.other_core()).wait_send()

    gather()
    g_send(0)
    gather_core()
    g_send(1)
    work(len(pieces))
    gather_y()
    g_send(2)
    gather_rest()
    g_send(3)
    project()
    for k, s in ends[:4]:
        g_wait(k, s)
    finish_conv()
    for k, s in ends[4:]:
        g_wait(k, s)
    g_own()
    g_other()
    drain()


def write_kernel(count, *refs):
    sources, targets, done = refs[:count], refs[count:2 * count], refs[2 * count]
    copies = [pltpu.make_async_copy(sources[n], targets[n], done.at[n]) for n in range(count)]
    for copy in copies:
        copy.start()
    for copy in copies:
        copy.wait()


def in_vmem(count):
    return [pl.BlockSpec(memory_space=pltpu.VMEM)] * count


def in_hbm(count):
    return [pl.BlockSpec(memory_space=pltpu.HBM)] * count


def fused(cotangent, stream, routes, route_weights, gate, up, down, outer, inner, given, taps,
          out_weight, experts, capacity):
    tokens, model = stream.shape
    units = gate.shape[1]
    channels = outer.shape[1]
    width = model // 4
    slice_width = model // (2 * experts)
    border, tail_rows = min(8, tokens), min(16, tokens)
    cut = capacity // 2 // 16 * 16
    rest = capacity - cut
    bf16, f32 = jnp.bfloat16, jnp.float32
    n = experts
    slots = 2 * capacity
    gate_shape = jax.ShapeDtypeStruct((model, units), bf16)
    own = jax.ShapeDtypeStruct((tokens, channels), bf16)
    outs = (
        gate_shape, gate_shape, jax.ShapeDtypeStruct((units, model), bf16),
        jax.ShapeDtypeStruct((slice_width, channels), f32), own, own, own,
    )
    half = (n, 2, 2, capacity, width)
    scratch = [
        ((2, tokens), jnp.int32), ((2, tokens), f32), ((2, tokens, model), bf16),
        ((n * capacity, tokens), bf16), ((n, capacity, 1), f32),
        ((model, units), bf16), ((model, units), bf16), ((units, model), bf16),
        ((tokens, channels), bf16), ((tokens, channels), bf16), ((tokens, channels), bf16),
        ((3, channels), bf16), ((model, channels), bf16),
        ((2, n, capacity, width), bf16), ((n, 2, capacity, model), bf16),
        ((n, 2, capacity, model), bf16), ((slots, units), f32), ((slots, units), f32),
        ((n, slots, units), bf16), ((n, slots, 2 * units), bf16),
        (half, bf16), (half, bf16), (half, bf16), (half, bf16),
        ((n, 2, cut, width), bf16), ((n, 2, rest, width), bf16),
        ((n, 2, cut, width), bf16), ((n, 2, rest, width), bf16),
        ((n, cut, width), bf16), ((n, rest, width), bf16),
        ((n, capacity, width), bf16), ((n, capacity, width), bf16),
        ((tokens, model), bf16), ((2, n, 2, tokens // 2, slice_width), bf16),
        ((2, n, 2, tokens // 2, channels), bf16), ((tokens, channels), f32),
        ((tail_rows, channels), f32), ((tail_rows, channels), f32),
        ((tokens + border, channels), f32), ((border, channels), f32),
    ]
    sems = [pltpu.SemaphoreType.DMA((12,)), pltpu.SemaphoreType.DMA((len(SEMS),))]
    sems += [pltpu.SemaphoreType.DMA(shape_of(n)) for shape_of in SEMS.values()]
    made = pl.pallas_call(
        functools.partial(fused_kernel, experts, capacity),
        out_shape=tuple(pltpu.VMEM(out.shape, out.dtype) for out in outs),
        in_specs=in_hbm(12),
        out_specs=tuple(in_vmem(7)),
        scratch_shapes=[pltpu.VMEM(*s) for s in scratch] + sems,
        compiler_params=pltpu.CompilerParams(
            collective_id=0, has_side_effects=True, vmem_limit_bytes=48 * 1024 * 1024
        ),
        name="fused",
    )(*[
        pltpu.with_memory_space_constraint(value, pltpu.HBM)
        for value in (
            routes.T, route_weights.T, stream, cotangent, gate, up, down, outer, inner, given,
            taps, out_weight,
        )
    ])
    written = pl.pallas_call(
        functools.partial(write_kernel, len(outs)),
        out_shape=outs,
        in_specs=in_vmem(len(outs)),
        out_specs=tuple(in_hbm(len(outs))),
        scratch_shapes=[pltpu.SemaphoreType.DMA((len(outs),))],
        compiler_params=pltpu.CompilerParams(vmem_limit_bytes=1024 * 1024),
        name="write",
    )(*made)
    return tuple(out[None] for out in written[:3]) + tuple(written[3:])


def per_device(
    cotangent,
    stream,
    routes,
    route_weights,
    gate_weight,
    up_weight,
    down_weight,
    outer_gate,
    inner_gate,
    conv_input,
    conv_taps,
    out_weight,
):
    groups = lax.axis_size("sp")
    tp_count = lax.axis_size("tp")
    experts = groups // 2
    tok_rows = stream.shape[0]
    model_width = stream.shape[1]
    capacity = 3 * tok_rows // experts
    slot_total = experts * capacity
    contract_first = (((0,), (0,)), ((), ()))
    contract_last = (((1,), (1,)), ((), ()))
    block_width = model_width // tp_count
    slots = groups * capacity
    even = experts == tp_count == 4
    if even and capacity % 32 == 0 and block_width % 128 == 0:
        return fused(
            cotangent, stream, routes, route_weights, gate_weight[0], up_weight[0],
            down_weight[0], outer_gate, inner_gate, conv_input, conv_taps, out_weight,
            experts, capacity,
        )
    taps = conv_taps.astype(jnp.float32)
    outer_f = outer_gate.astype(jnp.float32)
    inner_f = inner_gate.astype(jnp.float32)
    input_f = conv_input.astype(jnp.float32)
    mixed = inner_f * input_f
    flat_routes = routes.reshape(-1)
    choose = (flat_routes[:, None] == jnp.arange(experts, dtype=jnp.int32)[None, :]).astype(
        jnp.int32
    )
    before = jnp.cumsum(choose, axis=0) - choose
    slot_place = flat_routes * capacity + jnp.sum(before * choose, axis=1)
    slot_table = (jnp.arange(slot_total, dtype=jnp.int32)[:, None] == slot_place[None, :]).astype(
        jnp.float32
    )
    select = jnp.sum(slot_table.reshape(slot_total, tok_rows, 2), axis=2).astype(jnp.bfloat16)
    slot_weight = jnp.sum(slot_table * route_weights.reshape(-1)[None, :], axis=1)
    offset = lax.axis_index("tp") * block_width
    rows_part = lax.dynamic_slice_in_dim(stream, offset, block_width, 1)
    cot_part = lax.dynamic_slice_in_dim(cotangent, offset, block_width, 1)
    sent_rows = jnp.dot(select, rows_part, preferred_element_type=jnp.float32).astype(jnp.bfloat16)
    sent_cot = (
        jnp.dot(select, cot_part, preferred_element_type=jnp.float32) * slot_weight[:, None]
    ).astype(jnp.bfloat16)
    sent_rows = jnp.repeat(sent_rows.reshape(experts, capacity, -1), 2, axis=0)
    sent_cot = jnp.repeat(sent_cot.reshape(experts, capacity, -1), 2, axis=0)
    recv_rows, recv_cot = (
        lax.all_to_all(sent_rows, "sp", split_axis=0, concat_axis=0, tiled=True),
        lax.all_to_all(sent_cot, "sp", split_axis=0, concat_axis=0, tiled=True),
    )
    recv_rows, recv_cot = (
        lax.all_gather(recv_rows, "tp", axis=2, tiled=True),
        lax.all_gather(recv_cot, "tp", axis=2, tiled=True),
    )
    routed_rows = recv_rows.reshape(slots, model_width)
    routed_cot = recv_cot.reshape(slots, model_width)
    earlier = from_behind(mixed[-2:], "sp", 1)
    gate_local = gate_weight[0]
    up_local = up_weight[0]
    down_local = down_weight[0]
    gate_pre = jnp.dot(routed_rows, gate_local, preferred_element_type=jnp.float32)
    up_pre = jnp.dot(routed_rows, up_local, preferred_element_type=jnp.float32)
    hidden_grad = lax.dot_general(
        routed_cot, down_local, contract_last, preferred_element_type=jnp.float32
    )
    sigma = jax.nn.sigmoid(gate_pre)
    silu_gate = gate_pre * sigma
    hidden = (silu_gate * up_pre).astype(jnp.bfloat16)
    up_delta = (hidden_grad * silu_gate).astype(jnp.bfloat16)
    gate_delta = (hidden_grad * up_pre * sigma * (1.0 + gate_pre * (1.0 - sigma))).astype(
        jnp.bfloat16
    )
    row_partial = lax.dot_general(
        gate_delta, gate_local, contract_last, preferred_element_type=jnp.float32
    )
    row_partial = row_partial + lax.dot_general(
        up_delta, up_local, contract_last, preferred_element_type=jnp.float32
    )
    padded = jnp.concatenate([earlier, mixed], axis=0)
    conv_sum = taps[0] * padded[:-2] + taps[1] * padded[1:-1] + taps[2] * padded[2:]
    conv_out = (outer_f * conv_sum).astype(jnp.bfloat16)
    gate_grad = lax.dot_general(
        routed_rows, gate_delta, contract_first, preferred_element_type=jnp.float32
    ).astype(jnp.bfloat16)[None]
    up_grad = lax.dot_general(
        routed_rows, up_delta, contract_first, preferred_element_type=jnp.float32
    ).astype(jnp.bfloat16)[None]
    down_grad = lax.dot_general(
        hidden, routed_cot, contract_first, preferred_element_type=jnp.float32
    ).astype(jnp.bfloat16)[None]
    half_sums = lax.psum_scatter(
        row_partial.astype(jnp.bfloat16), "tp", scatter_dimension=1, tiled=True
    ).astype(jnp.float32)
    block_width = half_sums.shape[1]
    half_grad = half_sums.reshape(groups, capacity, block_width).astype(jnp.bfloat16)
    returned = lax.all_to_all(half_grad, "sp", split_axis=0, concat_axis=0, tiled=True)
    returned = returned.reshape(experts, 2, capacity, block_width)
    select_three = select.reshape(experts, capacity, tok_rows)
    moe_part = jnp.einsum(
        "ecr,emcd->rd", select_three, returned, preferred_element_type=jnp.float32
    ).astype(jnp.bfloat16)
    moe_grad = lax.all_gather(moe_part, "tp", axis=1, tiled=True)
    stream_grad = (cotangent.astype(jnp.float32) + moe_grad.astype(jnp.float32)).astype(
        jnp.bfloat16
    )
    out_grad = lax.psum_scatter(
        lax.dot_general(
            stream_grad, conv_out, contract_first, preferred_element_type=jnp.float32
        ).astype(jnp.bfloat16),
        "sp",
        scatter_dimension=0,
        tiled=True,
    ).astype(jnp.float32)
    conv_grad = jnp.dot(stream_grad, out_weight, preferred_element_type=jnp.float32)
    outer_grad = (conv_grad * conv_sum).astype(jnp.bfloat16)
    scaled = conv_grad * outer_f
    later = from_behind(scaled[:2], "sp", -1)
    extended = jnp.concatenate([scaled, later], axis=0)
    mixed_grad = taps[2] * extended[:-2] + taps[1] * extended[1:-1] + taps[0] * extended[2:]
    inner_grad = (mixed_grad * input_f).astype(jnp.bfloat16)
    input_grad = (mixed_grad * inner_f).astype(jnp.bfloat16)
    return (gate_grad, up_grad, down_grad, out_grad, outer_grad, inner_grad, input_grad)


def solution(mesh):
    placed = (
        P("sp", None),
        P("sp", None),
        P("sp", None),
        P("sp", None),
        P("sp", None, "tp"),
        P("sp", None, "tp"),
        P("sp", "tp", None),
        P("sp", "tp"),
        P("sp", "tp"),
        P("sp", "tp"),
        P(None, "tp"),
        P(None, "tp"),
    )
    return jax.shard_map(
        per_device,
        mesh=mesh,
        in_specs=placed,
        out_specs=(
            P("sp", None, "tp"),
            P("sp", None, "tp"),
            P("sp", "tp", None),
            P("sp", "tp"),
            P("sp", "tp"),
            P("sp", "tp"),
            P("sp", "tp"),
        ),
        check_vma=False,
    )
```

```python
import functools

import jax
import jax.numpy as jnp
from jax import lax
from jax.experimental import pallas as pl
from jax.experimental.pallas import tpu as pltpu
from jax.sharding import PartitionSpec as P


def from_behind(block, axis, distance):
    devices = range(lax.axis_size(axis))
    route = [(i - distance, i) for i in devices if i - distance in devices]
    return lax.ppermute(block, axis, route)


def remote(src, dst, sent, landed, device):
    return pltpu.make_async_remote_copy(
        src_ref=src,
        dst_ref=dst,
        send_sem=sent,
        recv_sem=landed,
        device_id=device,
        device_id_type=pl.DeviceIdType.MESH,
    )


class Seat:
    def __init__(self, experts):
        self.sp = lax.axis_index("sp")
        self.tp = lax.axis_index("tp")
        self.x = lax.rem(self.sp, 2)
        self.z = self.sp // 2
        self.c = lax.rem(self.tp, 2)
        self.y = self.tp // 2
        self.experts = experts

    def plane(self, k):
        number, weight = 0, 1
        while weight < self.experts:
            bit = lax.rem(self.z // weight, 2)
            number = number + weight * (1 - bit if k // weight % 2 else bit)
            weight *= 2
        return number

    def between(self, plane):
        number, weight = 0, 1
        while weight < self.experts:
            number = number + weight * lax.rem(self.z // weight + plane // weight, 2)
            weight *= 2
        return number

    def over_z(self, k, swap=0):
        return (self.plane(k) * 2 + (1 - self.x if swap else self.x), self.tp)

    def over_x(self):
        return (self.z * 2 + 1 - self.x, self.tp)

    def over_y(self):
        return (self.sp, (1 - self.y) * 2 + self.c)

    def other_core(self):
        return (self.sp, self.y * 2 + 1 - self.c)

    def next_tokens(self, distance):
        groups = 2 * self.experts
        return (lax.rem(self.sp + groups + distance, groups), self.tp)


SEMS = {
    "z": lambda n: (2, n), "x": lambda n: (2, n), "y": lambda n: (2, n), "d": lambda n: (2, n),
    "c0": lambda n: (2,), "c": lambda n: (2, n), "r1": lambda n: (n,), "r2": lambda n: (n, 2),
    "r3": lambda n: (n, 2), "r4": lambda n: (1,), "ag": lambda n: (3,), "g": lambda n: (n, 2),
    "gc": lambda n: (1,), "cz": lambda n: (1,), "cx": lambda n: (1,), "h0": lambda n: (1,),
    "h1": lambda n: (1,),
}

FIRST = (((0,), (0,)), ((), ()))
LAST = (((1,), (1,)), ((), ()))


def fused_kernel(experts, capacity, *refs):
    refs = list(refs)

    def take(count):
        got = refs[:count]
        del refs[:count]
        return got

    (routes_hbm, weights_hbm, stream_hbm, given_hbm, gate_hbm, up_hbm, down_hbm, outer_hbm,
     inner_hbm, input_hbm, taps_hbm, ow_hbm) = take(12)
    (gate_grad, up_grad, down_grad, out_grad, outer_grad, inner_grad, input_grad) = take(7)
    (routes_ref, weights_ref, block, sel, slot_weight, gate, up, down, outer, inner, given, taps, ow,
     send, rows, cots, gp_ref, up_ref, hid, delta, part, mine_part, a_ref, acc, b1a, b1b, acc2a,
     acc2b, b2a, b2b, fin, ret, sg, g_ref, c_ref, sum_ref, tail_ref, early, ext,
     late) = take(40)
    load_sem, sent_sem = take(2)
    names = list(SEMS)
    sem = dict(zip(names, take(len(names))))
    seat = Seat(experts)
    n_k = experts
    tokens, model = block.shape[1:]
    width = send.shape[3]
    units = gate.shape[1]
    cut = capacity // 2 // 16 * 16
    places = (rows, cots)
    slots = 2 * capacity
    f32, bf16 = jnp.float32, jnp.bfloat16

    barrier = pltpu.get_barrier_semaphore()
    peers = [seat.over_z(k, s) for k in range(n_k) for s in range(2) if k or s]
    peers += [seat.over_y(), seat.other_core()]

    pairs = (
        (routes_hbm, routes_ref), (weights_hbm, weights_ref), (stream_hbm, block.at[0]),
        (given_hbm, block.at[1]), (inner_hbm, inner), (input_hbm, given), (gate_hbm, gate),
        (up_hbm, up), (down_hbm, down), (outer_hbm, outer), (taps_hbm, taps), (ow_hbm, ow),
    )
    loads = [pltpu.make_async_copy(s, d, load_sem.at[n]) for n, (s, d) in enumerate(pairs)]
    for load in loads:
        load.start()
    for peer in peers:
        pl.semaphore_signal(barrier, inc=1, device_id=peer, device_id_type=pl.DeviceIdType.MESH)

    def push(src, dst, name, at, device):
        remote(src, dst, sent_sem.at[names.index(name)], sem[name].at[at], device).start()

    def landed(spot, name, at):
        remote(spot, spot, sent_sem.at[0], sem[name].at[at], seat.other_core()).wait_recv()

    def cols(tp):
        return pl.ds(pl.multiple_of(tp * width, width), width)

    def total(*terms):
        value = terms[0].astype(f32)
        for term in terms[1:]:
            value = value + term.astype(f32)
        return value.astype(bf16)

    my_cols = cols(seat.tp)
    y_cols = cols((1 - seat.y) * 2 + seat.c)
    core_cols = [cols(seat.y * 2 + 1 - seat.c), cols((1 - seat.y) * 2 + 1 - seat.c)]

    tail_rows = tail_ref.shape[0]
    edge = slice(tokens - tail_rows, tokens)

    def send_halo():
        loads[4].wait()
        loads[5].wait()
        tail_ref[...] = inner[edge, :].astype(f32) * given[edge, :].astype(f32)
        pl.semaphore_wait(barrier, len(peers))

        @pl.when(seat.sp < 2 * n_k - 1)
        def _():
            push(tail_ref, early, "h0", 0, seat.next_tokens(1))

    loads[0].wait()
    loads[1].wait()
    place_of = lax.broadcasted_iota(jnp.int32, (n_k, tokens), 0)
    number = jnp.zeros((n_k, tokens), jnp.int32)
    for k in range(n_k):
        number = jnp.where(place_of == k, seat.plane(k), number)
    named = [routes_ref[j:j + 1, :] == number for j in range(2)]
    member = jnp.where(named[0] | named[1], 1.0, 0.0)
    share = jnp.where(named[0], weights_ref[0:1, :], 0.0) + jnp.where(
        named[1], weights_ref[1:2, :], 0.0
    )
    sooner = lax.broadcasted_iota(jnp.int32, (tokens, tokens), 0) < lax.broadcasted_iota(
        jnp.int32, (tokens, tokens), 1
    )
    rank = jnp.dot(
        member.astype(bf16), jnp.where(sooner, 1.0, 0.0).astype(bf16), preferred_element_type=f32
    )
    slot = lax.broadcasted_iota(jnp.int32, (capacity, tokens), 0).astype(f32)
    for k in range(n_k):
        chosen = jnp.where(slot == rank[k:k + 1], member[k:k + 1], 0.0)
        slot_weight[k] = jnp.sum(chosen * share[k:k + 1], axis=1, keepdims=True)
        sel[k * capacity:(k + 1) * capacity, :] = chosen.astype(bf16)

    def pick(kind, k, span):
        got = jnp.dot(
            sel[k * capacity:(k + 1) * capacity, :], block[kind, :, span],
            preferred_element_type=f32,
        )
        if kind:
            got = got * slot_weight[k]
        return got.astype(bf16)

    order = list(range(n_k))

    def fill(k, kind):
        send[kind, k] = pick(kind, k, my_cols)

    def launch(k, kind):
        plane = seat.between(k)
        push(send.at[kind, k], places[kind].at[k, seat.x, :, my_cols], "z", (kind, k),
             (plane * 2 + seat.x, seat.tp))

    def fill_own(kind):
        for tp in range(model // width):
            span = slice(tp * width, (tp + 1) * width)
            places[kind][0, seat.x, :, span] = pick(kind, 0, span)

    def spot_of(item, x, span):
        kind, k = item
        return places[kind].at[k, x, :, span]

    def half_of(item, x, span, j):
        kind, k = item
        edge_at = capacity // 3 // 16 * 16
        part_rows = pl.ds(edge_at, capacity - edge_at) if j else pl.ds(0, edge_at)
        return places[kind].at[k, x, part_rows, span]

    ox = 1 - seat.x

    def to_core(spot, item):
        kind, k = item
        push(spot, spot, "c" if k else "c0", item if k else kind, seat.other_core())

    def s1(item):
        kind, k = item
        if k == 0:
            spot = spot_of(item, seat.x, my_cols)
            push(spot, spot, "x", item, seat.over_x())
        else:
            spot = spot_of(item, seat.x, my_cols)
            landed(spot, "z", item)
            push(spot, spot, "x", item, seat.over_x())
            push(spot, spot, "y", item, seat.over_y())
            push(spot, spot, "c", item, seat.other_core())

    def s2x(item):
        kind, k = item
        spot = spot_of(item, ox, my_cols)
        landed(spot, "x", item)
        if k == 0:
            push(spot, spot, "y", item, seat.over_y())
        else:
            part_spot = half_of(item, ox, my_cols, 0)
            push(part_spot, part_spot, "d", item, seat.over_y())
        to_core(spot, item)

    def s2y(item):
        spot = spot_of(item, seat.x, y_cols)
        landed(spot, "y", item)
        part_spot = half_of(item, seat.x, y_cols, 1)
        push(part_spot, part_spot, "d", item, seat.over_x())
        to_core(spot, item)

    def s3(item):
        kind, k = item
        spot = spot_of(item, ox, y_cols)
        if k == 0:
            landed(spot, "y", item)
        else:
            landed(spot, "d", item)
        to_core(spot, item)

    def s4(item):
        kind, k = item
        if k == 0:
            landed(rows.at[0, :, :, 0:width], "c0", kind)
        else:
            landed(rows.at[k, :, :, 0:2 * width], "c", item)

    tile = 256 if units % 256 == 0 else units

    def pre(k):
        lhs = rows[k].reshape(slots, model)
        for at in range(0, units, tile):
            gp_ref[int(k == 1), :, at:at + tile] = jnp.dot(lhs, gate[:, at:at + tile], preferred_element_type=f32)
            up_ref[int(k == 1), :, at:at + tile] = jnp.dot(lhs, up[:, at:at + tile], preferred_element_type=f32)

    def mid(k):
        lhs = cots[k].reshape(slots, model)
        for at in range(0, units, tile):
            span = slice(at, at + tile)
            grad = lax.dot_general(lhs, down[span, :], LAST, preferred_element_type=f32)
            gate_pre, up_pre = gp_ref[int(k == 1), :, span], up_ref[int(k == 1), :, span]
            sigma = jax.nn.sigmoid(gate_pre)
            silu = gate_pre * sigma
            hid[k, :, span] = (silu * up_pre).astype(bf16)
            delta[k, :, units + at:units + at + tile] = (grad * silu).astype(bf16)
            delta[k, :, span] = (grad * up_pre * sigma * (1.0 + gate_pre * (1.0 - sigma))).astype(bf16)

    def post(k, y, mine):
        out = mine_part if mine else part
        core = seat.c if mine else 1 - seat.c
        for at in range(0, width, tile):
            first = pl.ds(pl.multiple_of((y * 2 + core) * width + at, tile), tile)
            value = lax.dot_general(
                delta[k, :, :units], gate[first, :], LAST, preferred_element_type=f32
            )
            value = value + lax.dot_general(
                delta[k, :, units:], up[first, :], LAST, preferred_element_type=f32
            )
            out[k, y, :, :, at:at + tile] = value.astype(bf16).reshape(2, capacity, tile)
        if not mine:
            push(part.at[k, y], a_ref.at[k, y], "r1", k, seat.other_core())

    def r2(k):
        landed(a_ref.at[k], "r1", k)
        for y in range(2):
            acc[k, y] = total(mine_part[k, y], a_ref[k, y])
        push(acc.at[k, :, ox, pl.ds(0, cut), :], b1a.at[k], "r2", (k, 0), seat.over_x())
        push(acc.at[k, 1 - seat.y, :, pl.ds(cut, capacity - cut), :], b1b.at[k], "r2", (k, 1),
             seat.over_y())

    def r3(k):
        landed(b1a.at[k], "r2", (k, 0))
        for y in range(2):
            acc2a[k, y] = total(acc[k, y, seat.x, 0:cut, :], b1a[k, y])
        push(acc2a.at[k, 1 - seat.y], b2a.at[k], "r3", (k, 0), seat.over_y())
        landed(b1b.at[k], "r2", (k, 1))
        for x in range(2):
            acc2b[k, x] = total(acc[k, seat.y, x, cut:capacity, :], b1b[k, x])
        push(acc2b.at[k, ox], b2b.at[k], "r3", (k, 1), seat.over_x())

    def r4(k):
        landed(b2a.at[k], "r3", (k, 0))
        landed(b2b.at[k], "r3", (k, 1))
        out = fin.at[k] if k else ret.at[0]
        out[0:cut, :] = total(acc2a[k, seat.y], b2a[k])
        out[cut:capacity, :] = total(acc2b[k, seat.x], b2b[k])
        if k:
            push(fin.at[k], ret.at[k], "r4", 0, seat.over_z(k))

    step = 256 if model % 256 == 0 else model
    pieces = [(0, at) for at in range(0, model, step)] + [(1, at) for at in range(0, model, 2 * step)]

    def work(count):
        for _ in range(min(count, len(pieces))):
            kind, at = pieces.pop(0)
            if kind == 0:
                lhs = rows[:, :, :, at:at + step].reshape(n_k * slots, step)
                for half in range(2):
                    out = up_grad if half else gate_grad
                    out[at:at + step, :] = lax.dot_general(
                        lhs, delta[:, :, half * units:(half + 1) * units].reshape(n_k * slots, units),
                        FIRST, preferred_element_type=f32,
                    ).astype(bf16)
            else:
                rhs = cots[:, :, :, at:at + 2 * step].reshape(n_k * slots, 2 * step)
                down_grad[:, at:at + 2 * step] = lax.dot_general(
                    hid[...].reshape(n_k * slots, units), rhs, FIRST, preferred_element_type=f32
                ).astype(bf16)

    share_rows = tokens // 2
    slice_width = g_ref.shape[4]

    def convolve():
        loads[10].wait()
        loads[9].wait()
        @pl.when(seat.sp > 0)
        def _():
            landed(early, "h0", 0)

        @pl.when(seat.sp == 0)
        def _():
            early[...] = jnp.zeros_like(early)

        earlier = early[tail_rows - 2:tail_rows, :]
        mixed = inner[...].astype(f32) * given[...].astype(f32)
        padded = jnp.concatenate([earlier, mixed], axis=0)
        t = taps[...].astype(f32)
        value = t[0:1] * padded[0:tokens] + t[1:2] * padded[1:tokens + 1]
        value = value + t[2:3] * mixed
        sum_ref[...] = value
        value = (outer[...].astype(f32) * value).astype(bf16)
        for j in range(2):
            c_ref[j, 0, 0] = value[j * share_rows:(j + 1) * share_rows]

    def spread_z():
        for k in range(1, n_k):
            push(c_ref.at[:, 0, 0], c_ref.at[:, k, 0], "cz", 0, seat.over_z(k))

    def spread_x():
        landed(c_ref.at[:, 1:n_k, 0], "cz", 0)
        for k in range(n_k):
            push(c_ref.at[:, k, 0], c_ref.at[:, k, 1], "cx", 0, seat.over_x())

    near, far, cross = 1, 2, 3
    items = [(kind, k) for k in (0, near, cross, far) for kind in range(2)]

    def away(k):
        post(k, 0, False)
        post(k, 1, False)

    def keep(k):
        post(k, 0, True)
        post(k, 1, True)

    border = late.shape[0]
    ends = [(k, s) for k in order for s in range(2) if k or s]

    def gather():
        landed(ret.at[1:n_k], "r4", 0)
        moe = lax.dot_general(
            sel[...], ret[...].reshape(n_k * capacity, width), FIRST, preferred_element_type=f32
        )
        sg[:, my_cols] = total(block[1, :, my_cols], moe.astype(bf16))
        spot = sg.at[:, my_cols]
        push(spot, spot, "ag", 0, seat.over_y())
        push(spot, spot, "ag", 1, seat.other_core())

    def flip(bits):
        number, weight = 0, 1
        while weight < n_k:
            number = number + weight * lax.rem(bits // weight + seat.tp // weight, 2)
            weight *= 2
        return number

    def g_half(k, swap, core):
        return g_ref.at[core, k, swap]

    mine_half = pl.ds(pl.multiple_of(seat.c * share_rows, share_rows), share_rows)

    def g_send(j):
        plane = flip(j)
        k = seat.between(plane)
        for s in range(2):
            d = plane * 2 + (ox if s else seat.x)
            src = sg.at[mine_half, pl.ds(pl.multiple_of(d * slice_width, slice_width), slice_width)]
            if s:
                push(src, g_half(k, s, seat.c), "g", (k, s), (d, seat.tp))
            else:
                @pl.when(k > 0)
                def _():
                    push(src, g_half(k, s, seat.c), "g", (k, s), (d, seat.tp))

    def gather_core():
        landed(sg.at[:, core_cols[0]], "ag", 1)

    def gather_y():
        spot = sg.at[:, y_cols]
        landed(spot, "ag", 0)
        push(spot, spot, "ag", 2, seat.other_core())

    def gather_rest():
        landed(sg.at[:, core_cols[1]], "ag", 2)

    def project():
        conv_grad = jnp.dot(sg[...], ow[...], preferred_element_type=f32)
        ext[0:tokens, :] = conv_grad * outer[...].astype(f32)

        @pl.when(seat.sp > 0)
        def _():
            push(ext.at[0:border, :], late, "h1", 0, seat.next_tokens(-1))

        outer_grad[...] = (conv_grad * sum_ref[...]).astype(bf16)
        own = pl.ds(pl.multiple_of(seat.sp * slice_width, slice_width), slice_width)
        for j in range(2):
            g_ref[j, 0, 0] = sg[j * share_rows:(j + 1) * share_rows, own]

    def finish_conv():
        @pl.when(seat.sp < 2 * n_k - 1)
        def _():
            landed(late, "h1", 0)
            ext[tokens:tokens + border, :] = late[...]

        @pl.when(seat.sp == 2 * n_k - 1)
        def _():
            ext[tokens:tokens + border, :] = jnp.zeros_like(late)

        t = taps[...].astype(f32)
        mixed_grad = t[2:3] * ext[0:tokens, :]
        mixed_grad = mixed_grad + t[1:2] * ext[1:tokens + 1, :]
        mixed_grad = mixed_grad + t[0:1] * ext[2:tokens + 2, :]
        inner_grad[...] = (mixed_grad * given[...].astype(f32)).astype(bf16)
        input_grad[...] = (mixed_grad * inner[...].astype(f32)).astype(bf16)

    def g_wait(k, s):
        spot = g_half(k, s, seat.c)
        landed(spot, "g", (k, s))
        push(spot, spot, "gc", 0, seat.other_core())

    def g_add(core):
        rows_of = 2 * n_k * share_rows
        return lax.dot_general(
            g_ref[core].reshape(rows_of, slice_width), c_ref[core].reshape(rows_of, -1), FIRST,
            preferred_element_type=f32,
        )

    def g_own():
        landed(c_ref.at[:, :, 1], "cx", 0)
        out_grad[...] = g_add(seat.c)

    def g_other():
        landed(sg.at[0:share_rows, 0:len(ends) * slice_width], "gc", 0)
        out_grad[...] += g_add(1 - seat.c)

    def drain():
        pieces_sent = sg.at[0:share_rows, 0:len(ends) * slice_width]
        spans = {
            "z": send.at[:, 1:n_k], "x": rows.at[:, :, :, 0:width], "y": rows.at[:, :, :, 0:width],
            "d": send.at[:, 1:n_k], "c0": rows.at[0:2, :, :, 0:width], "c": rows.at[0:n_k - 1],
            "r1": part, "r2": part.at[:, 0], "r3": part.at[:, 0, 0], "r4": part.at[0:n_k - 1, 0, 0],
            "ag": sg.at[:, 0:3 * width], "g": pieces_sent, "gc": pieces_sent,
            "cz": c_ref.at[:, 1:n_k, 0], "cx": c_ref.at[:, :, 0], "h0": tail_ref,
            "h1": ext.at[0:border, :],
        }

        def wait_sent(name):
            span, at = spans[name], names.index(name)
            remote(span, span, sent_sem.at[at], load_sem.at[0], seat.other_core()).wait_send()

        for name in names:
            if name == "h0":
                pl.when(seat.sp < 2 * n_k - 1)(functools.partial(wait_sent, name))
            elif name == "h1":
                pl.when(seat.sp > 0)(functools.partial(wait_sent, name))
            else:
                wait_sent(name)

    inner_plane = (seat.z + seat.z // 2) % 2

    def first_wave(kind):
        launch(near + inner_plane * (cross - near), kind)

        @pl.when(inner_plane == 1)
        def _():
            launch(near, kind)

    def second_wave():
        for kind in range(2):
            launch(cross - inner_plane * (cross - far), kind)

    def third_wave():
        @pl.when(inner_plane == 0)
        def _():
            for kind in range(2):
                launch(far, kind)

    loads[2].wait()
    fill(near, 0)
    fill(cross, 0)
    fill_own(0)
    send_halo()
    s1(items[0])
    first_wave(0)
    loads[3].wait()
    fill(near, 1)
    fill(cross, 1)
    first_wave(1)
    fill_own(1)
    s1(items[1])
    fill(far, 0)
    fill(far, 1)
    s1(items[2])
    s2x(items[0])
    second_wave()
    s1(items[3])
    s2y(items[2])
    third_wave()
    s2x(items[1])
    s2x(items[2])
    s2x(items[3])
    s1(items[4])
    s2y(items[3])
    s3(items[0])
    s1(items[5])
    s3(items[1])
    s4(items[0])
    s3(items[2])
    s2x(items[4])
    for load in loads[6:9]:
        load.wait()
    pre(0)
    s1(items[6])
    s2y(items[4])
    s4(items[2])
    s4(items[1])
    convolve()
    s3(items[3])
    mid(0)
    s2x(items[5])
    post(0, 1, True)
    post(0, 0, True)
    s4(items[3])
    s2y(items[5])
    post(0, 1, False)
    pre(near)
    s1(items[7])
    spread_z()
    s3(items[4])
    mid(near)
    post(0, 0, False)
    s2y(items[6])
    post(near, 1, True)
    s2x(items[6])
    s3(items[5])
    s4(items[4])
    pre(cross)
    post(near, 0, False)
    r2(0)
    post(near, 0, True)
    s2x(items[7])
    s2y(items[7])
    post(near, 1, False)
    s3(items[6])
    s4(items[5])
    mid(cross)
    post(cross, 0, True)
    post(cross, 1, False)
    r2(near)
    s4(items[6])
    post(cross, 0, False)
    pre(far)
    s3(items[7])
    post(cross, 1, True)
    r2(cross)
    s4(items[7])
    r3(0)
    mid(far)
    r3(near)
    post(far, 1, False)
    post(far, 0, False)
    post(far, 0, True)
    post(far, 1, True)
    r3(cross)
    r2(far)
    r4(0)
    r4(near)
    work(2)
    r4(cross)
    work(1)
    r3(far)
    spread_x()
    work(3)
    r4(far)
    work(3)
    gather()
    g_send(0)
    work(3)
    loads[11].wait()
    gather_core()
    g_send(1)
    work(len(pieces))
    gather_y()
    g_send(2)
    gather_rest()
    g_send(3)
    project()
    for k, s in ends:
        g_wait(k, s)
    finish_conv()
    g_own()
    g_other()
    drain()


def write_kernel(count, *refs):
    sources, targets, done = refs[:count], refs[count:2 * count], refs[2 * count]
    for n in range(count):
        rows = sources[n].shape[0]
        step = rows // 8 if rows % 128 == 0 and rows > 256 else rows
        for at in range(0, rows, step):
            span = pl.ds(at, step)
            pltpu.make_async_copy(sources[n].at[span], targets[n].at[span], done.at[n]).start()
    for n in range(count):
        pltpu.make_async_copy(sources[n], targets[n], done.at[n]).wait()


def in_vmem(count):
    return [pl.BlockSpec(memory_space=pltpu.VMEM)] * count


def in_hbm(count):
    return [pl.BlockSpec(memory_space=pltpu.HBM)] * count


def fused(cotangent, stream, routes, route_weights, gate, up, down, outer, inner, given, taps,
          out_weight, experts, capacity):
    tokens, model = stream.shape
    units = gate.shape[1]
    channels = outer.shape[1]
    width = model // 4
    slice_width = model // (2 * experts)
    border, tail_rows = min(8, tokens), min(16, tokens)
    cut = capacity // 2 // 16 * 16
    rest = capacity - cut
    bf16, f32 = jnp.bfloat16, jnp.float32
    n = experts
    slots = 2 * capacity
    gate_shape = jax.ShapeDtypeStruct((model, units), bf16)
    own = jax.ShapeDtypeStruct((tokens, channels), bf16)
    outs = (
        gate_shape, gate_shape, jax.ShapeDtypeStruct((units, model), bf16),
        jax.ShapeDtypeStruct((slice_width, channels), f32), own, own, own,
    )
    half = (n, 2, 2, capacity, width)
    scratch = [
        ((2, tokens), jnp.int32), ((2, tokens), f32), ((2, tokens, model), bf16),
        ((n * capacity, tokens), bf16), ((n, capacity, 1), f32),
        ((model, units), bf16), ((model, units), bf16), ((units, model), bf16),
        ((tokens, channels), bf16), ((tokens, channels), bf16), ((tokens, channels), bf16),
        ((3, channels), bf16), ((model, channels), bf16),
        ((2, n, capacity, width), bf16), ((n, 2, capacity, model), bf16),
        ((n, 2, capacity, model), bf16), ((2, slots, units), f32), ((2, slots, units), f32),
        ((n, slots, units), bf16), ((n, slots, 2 * units), bf16),
        (half, bf16), (half, bf16), (half, bf16), (half, bf16),
        ((n, 2, cut, width), bf16), ((n, 2, rest, width), bf16),
        ((n, 2, cut, width), bf16), ((n, 2, rest, width), bf16),
        ((n, cut, width), bf16), ((n, rest, width), bf16),
        ((n, capacity, width), bf16), ((n, capacity, width), bf16),
        ((tokens, model), bf16), ((2, n, 2, tokens // 2, slice_width), bf16),
        ((2, n, 2, tokens // 2, channels), bf16), ((tokens, channels), f32),
        ((tail_rows, channels), f32), ((tail_rows, channels), f32),
        ((tokens + border, channels), f32), ((border, channels), f32),
    ]
    sems = [pltpu.SemaphoreType.DMA((12,)), pltpu.SemaphoreType.DMA((len(SEMS),))]
    sems += [pltpu.SemaphoreType.DMA(shape_of(n)) for shape_of in SEMS.values()]
    made = pl.pallas_call(
        functools.partial(fused_kernel, experts, capacity),
        out_shape=tuple(pltpu.VMEM(out.shape, out.dtype) for out in outs),
        in_specs=in_hbm(12),
        out_specs=tuple(in_vmem(7)),
        scratch_shapes=[pltpu.VMEM(*s) for s in scratch] + sems,
        compiler_params=pltpu.CompilerParams(
            collective_id=0, has_side_effects=True, vmem_limit_bytes=48 * 1024 * 1024
        ),
        name="fused",
    )(*[
        pltpu.with_memory_space_constraint(value, pltpu.HBM)
        for value in (
            routes.T, route_weights.T, stream, cotangent, gate, up, down, outer, inner, given,
            taps, out_weight,
        )
    ])
    written = pl.pallas_call(
        functools.partial(write_kernel, len(outs)),
        out_shape=outs,
        in_specs=in_vmem(len(outs)),
        out_specs=tuple(in_hbm(len(outs))),
        scratch_shapes=[pltpu.SemaphoreType.DMA((len(outs),))],
        compiler_params=pltpu.CompilerParams(vmem_limit_bytes=1024 * 1024),
        name="write",
    )(*made)
    return tuple(out[None] for out in written[:3]) + tuple(written[3:])


def per_device(
    cotangent,
    stream,
    routes,
    route_weights,
    gate_weight,
    up_weight,
    down_weight,
    outer_gate,
    inner_gate,
    conv_input,
    conv_taps,
    out_weight,
):
    groups = lax.axis_size("sp")
    tp_count = lax.axis_size("tp")
    experts = groups // 2
    tok_rows = stream.shape[0]
    model_width = stream.shape[1]
    capacity = 3 * tok_rows // experts
    slot_total = experts * capacity
    contract_first = (((0,), (0,)), ((), ()))
    contract_last = (((1,), (1,)), ((), ()))
    block_width = model_width // tp_count
    slots = groups * capacity
    even = experts == tp_count == 4
    if even and capacity % 32 == 0 and block_width % 128 == 0:
        return fused(
            cotangent, stream, routes, route_weights, gate_weight[0], up_weight[0],
            down_weight[0], outer_gate, inner_gate, conv_input, conv_taps, out_weight,
            experts, capacity,
        )
    taps = conv_taps.astype(jnp.float32)
    outer_f = outer_gate.astype(jnp.float32)
    inner_f = inner_gate.astype(jnp.float32)
    input_f = conv_input.astype(jnp.float32)
    mixed = inner_f * input_f
    flat_routes = routes.reshape(-1)
    choose = (flat_routes[:, None] == jnp.arange(experts, dtype=jnp.int32)[None, :]).astype(
        jnp.int32
    )
    before = jnp.cumsum(choose, axis=0) - choose
    slot_place = flat_routes * capacity + jnp.sum(before * choose, axis=1)
    slot_table = (jnp.arange(slot_total, dtype=jnp.int32)[:, None] == slot_place[None, :]).astype(
        jnp.float32
    )
    select = jnp.sum(slot_table.reshape(slot_total, tok_rows, 2), axis=2).astype(jnp.bfloat16)
    slot_weight = jnp.sum(slot_table * route_weights.reshape(-1)[None, :], axis=1)
    offset = lax.axis_index("tp") * block_width
    rows_part = lax.dynamic_slice_in_dim(stream, offset, block_width, 1)
    cot_part = lax.dynamic_slice_in_dim(cotangent, offset, block_width, 1)
    sent_rows = jnp.dot(select, rows_part, preferred_element_type=jnp.float32).astype(jnp.bfloat16)
    sent_cot = (
        jnp.dot(select, cot_part, preferred_element_type=jnp.float32) * slot_weight[:, None]
    ).astype(jnp.bfloat16)
    sent_rows = jnp.repeat(sent_rows.reshape(experts, capacity, -1), 2, axis=0)
    sent_cot = jnp.repeat(sent_cot.reshape(experts, capacity, -1), 2, axis=0)
    recv_rows, recv_cot = (
        lax.all_to_all(sent_rows, "sp", split_axis=0, concat_axis=0, tiled=True),
        lax.all_to_all(sent_cot, "sp", split_axis=0, concat_axis=0, tiled=True),
    )
    recv_rows, recv_cot = (
        lax.all_gather(recv_rows, "tp", axis=2, tiled=True),
        lax.all_gather(recv_cot, "tp", axis=2, tiled=True),
    )
    routed_rows = recv_rows.reshape(slots, model_width)
    routed_cot = recv_cot.reshape(slots, model_width)
    earlier = from_behind(mixed[-2:], "sp", 1)
    gate_local = gate_weight[0]
    up_local = up_weight[0]
    down_local = down_weight[0]
    gate_pre = jnp.dot(routed_rows, gate_local, preferred_element_type=jnp.float32)
    up_pre = jnp.dot(routed_rows, up_local, preferred_element_type=jnp.float32)
    hidden_grad = lax.dot_general(
        routed_cot, down_local, contract_last, preferred_element_type=jnp.float32
    )
    sigma = jax.nn.sigmoid(gate_pre)
    silu_gate = gate_pre * sigma
    hidden = (silu_gate * up_pre).astype(jnp.bfloat16)
    up_delta = (hidden_grad * silu_gate).astype(jnp.bfloat16)
    gate_delta = (hidden_grad * up_pre * sigma * (1.0 + gate_pre * (1.0 - sigma))).astype(
        jnp.bfloat16
    )
    row_partial = lax.dot_general(
        gate_delta, gate_local, contract_last, preferred_element_type=jnp.float32
    )
    row_partial = row_partial + lax.dot_general(
        up_delta, up_local, contract_last, preferred_element_type=jnp.float32
    )
    padded = jnp.concatenate([earlier, mixed], axis=0)
    conv_sum = taps[0] * padded[:-2] + taps[1] * padded[1:-1] + taps[2] * padded[2:]
    conv_out = (outer_f * conv_sum).astype(jnp.bfloat16)
    gate_grad = lax.dot_general(
        routed_rows, gate_delta, contract_first, preferred_element_type=jnp.float32
    ).astype(jnp.bfloat16)[None]
    up_grad = lax.dot_general(
        routed_rows, up_delta, contract_first, preferred_element_type=jnp.float32
    ).astype(jnp.bfloat16)[None]
    down_grad = lax.dot_general(
        hidden, routed_cot, contract_first, preferred_element_type=jnp.float32
    ).astype(jnp.bfloat16)[None]
    half_sums = lax.psum_scatter(
        row_partial.astype(jnp.bfloat16), "tp", scatter_dimension=1, tiled=True
    ).astype(jnp.float32)
    block_width = half_sums.shape[1]
    half_grad = half_sums.reshape(groups, capacity, block_width).astype(jnp.bfloat16)
    returned = lax.all_to_all(half_grad, "sp", split_axis=0, concat_axis=0, tiled=True)
    returned = returned.reshape(experts, 2, capacity, block_width)
    select_three = select.reshape(experts, capacity, tok_rows)
    moe_part = jnp.einsum(
        "ecr,emcd->rd", select_three, returned, preferred_element_type=jnp.float32
    ).astype(jnp.bfloat16)
    moe_grad = lax.all_gather(moe_part, "tp", axis=1, tiled=True)
    stream_grad = (cotangent.astype(jnp.float32) + moe_grad.astype(jnp.float32)).astype(
        jnp.bfloat16
    )
    out_grad = lax.psum_scatter(
        lax.dot_general(
            stream_grad, conv_out, contract_first, preferred_element_type=jnp.float32
        ).astype(jnp.bfloat16),
        "sp",
        scatter_dimension=0,
        tiled=True,
    ).astype(jnp.float32)
    conv_grad = jnp.dot(stream_grad, out_weight, preferred_element_type=jnp.float32)
    outer_grad = (conv_grad * conv_sum).astype(jnp.bfloat16)
    scaled = conv_grad * outer_f
    later = from_behind(scaled[:2], "sp", -1)
    extended = jnp.concatenate([scaled, later], axis=0)
    mixed_grad = taps[2] * extended[:-2] + taps[1] * extended[1:-1] + taps[0] * extended[2:]
    inner_grad = (mixed_grad * input_f).astype(jnp.bfloat16)
    input_grad = (mixed_grad * inner_f).astype(jnp.bfloat16)
    return (gate_grad, up_grad, down_grad, out_grad, outer_grad, inner_grad, input_grad)


def solution(mesh):
    placed = (
        P("sp", None),
        P("sp", None),
        P("sp", None),
        P("sp", None),
        P("sp", None, "tp"),
        P("sp", None, "tp"),
        P("sp", "tp", None),
        P("sp", "tp"),
        P("sp", "tp"),
        P("sp", "tp"),
        P(None, "tp"),
        P(None, "tp"),
    )
    return jax.shard_map(
        per_device,
        mesh=mesh,
        in_specs=placed,
        out_specs=(
            P("sp", None, "tp"),
            P("sp", None, "tp"),
            P("sp", "tp", None),
            P("sp", "tp"),
            P("sp", "tp"),
            P("sp", "tp"),
            P("sp", "tp"),
        ),
        check_vma=False,
    )
```

```python
import functools

import jax
import jax.numpy as jnp
from jax import lax
from jax.experimental import pallas as pl
from jax.experimental.pallas import tpu as pltpu
from jax.sharding import PartitionSpec as P


def from_behind(block, axis, distance):
    devices = range(lax.axis_size(axis))
    route = [(i - distance, i) for i in devices if i - distance in devices]
    return lax.ppermute(block, axis, route)


def remote(src, dst, sent, landed, device):
    return pltpu.make_async_remote_copy(
        src_ref=src,
        dst_ref=dst,
        send_sem=sent,
        recv_sem=landed,
        device_id=device,
        device_id_type=pl.DeviceIdType.MESH,
    )


class Seat:
    def __init__(self, experts):
        self.sp = lax.axis_index("sp")
        self.tp = lax.axis_index("tp")
        self.x = lax.rem(self.sp, 2)
        self.z = self.sp // 2
        self.c = lax.rem(self.tp, 2)
        self.y = self.tp // 2
        self.experts = experts

    def plane(self, k):
        number, weight = 0, 1
        while weight < self.experts:
            bit = lax.rem(self.z // weight, 2)
            number = number + weight * (1 - bit if k // weight % 2 else bit)
            weight *= 2
        return number

    def between(self, plane):
        number, weight = 0, 1
        while weight < self.experts:
            number = number + weight * lax.rem(self.z // weight + plane // weight, 2)
            weight *= 2
        return number

    def over_z(self, k, swap=0):
        return (self.plane(k) * 2 + (1 - self.x if swap else self.x), self.tp)

    def over_x(self):
        return (self.z * 2 + 1 - self.x, self.tp)

    def over_y(self):
        return (self.sp, (1 - self.y) * 2 + self.c)

    def other_core(self):
        return (self.sp, self.y * 2 + 1 - self.c)

    def next_tokens(self, distance):
        groups = 2 * self.experts
        return (lax.rem(self.sp + groups + distance, groups), self.tp)


SEMS = {
    "z": lambda n: (2, n), "x": lambda n: (2, n), "y": lambda n: (2, n), "d": lambda n: (2, n),
    "c0": lambda n: (2,), "c": lambda n: (2, n), "r1": lambda n: (n,), "r2": lambda n: (n, 4),
    "r3": lambda n: (n, 2), "r4": lambda n: (1,), "ag": lambda n: (3,), "g": lambda n: (n, 2),
    "gc": lambda n: (1,), "cz": lambda n: (1,), "cx": lambda n: (1,), "h0": lambda n: (1,),
    "h1": lambda n: (1,),
}

FIRST = (((0,), (0,)), ((), ()))
LAST = (((1,), (1,)), ((), ()))


def fused_kernel(experts, capacity, *refs):
    refs = list(refs)

    def take(count):
        got = refs[:count]
        del refs[:count]
        return got

    (routes_hbm, weights_hbm, stream_hbm, given_hbm, gate_hbm, up_hbm, down_hbm, outer_hbm,
     inner_hbm, input_hbm, taps_hbm, ow_hbm) = take(12)
    (gate_grad, up_grad, down_grad, out_grad, outer_grad, inner_grad, input_grad) = take(7)
    (routes_ref, weights_ref, block, sel, slot_weight, gate, up, down, outer, inner, given, taps, ow,
     send, rows, cots, gp_ref, up_ref, hid, delta, part, mine_part, a_ref, acc, b1a, b1b, acc2a,
     acc2b, b2a, b2b, fin, ret, sg, g_ref, c_ref, sum_ref, tail_ref, early, ext,
     late) = take(40)
    load_sem, sent_sem = take(2)
    names = list(SEMS)
    sem = dict(zip(names, take(len(names))))
    seat = Seat(experts)
    n_k = experts
    tokens, model = block.shape[1:]
    width = send.shape[3]
    units = gate.shape[1]
    cut = capacity // 2 // 16 * 16
    places = (rows, cots)
    slots = 2 * capacity
    f32, bf16 = jnp.float32, jnp.bfloat16

    barrier = pltpu.get_barrier_semaphore()
    peers = [seat.over_z(k, s) for k in range(n_k) for s in range(2) if k or s]
    peers += [seat.over_y(), seat.other_core()]

    pairs = (
        (routes_hbm, routes_ref), (weights_hbm, weights_ref), (stream_hbm, block.at[0]),
        (given_hbm, block.at[1]), (inner_hbm, inner), (input_hbm, given), (gate_hbm, gate),
        (up_hbm, up), (down_hbm, down), (outer_hbm, outer), (taps_hbm, taps), (ow_hbm, ow),
    )
    loads = [pltpu.make_async_copy(s, d, load_sem.at[n]) for n, (s, d) in enumerate(pairs)]
    for load in loads:
        load.start()
    for peer in peers:
        pl.semaphore_signal(barrier, inc=1, device_id=peer, device_id_type=pl.DeviceIdType.MESH)

    def push(src, dst, name, at, device):
        remote(src, dst, sent_sem.at[names.index(name)], sem[name].at[at], device).start()

    def landed(spot, name, at):
        remote(spot, spot, sent_sem.at[0], sem[name].at[at], seat.other_core()).wait_recv()

    def cols(tp):
        return pl.ds(pl.multiple_of(tp * width, width), width)

    def total(*terms):
        value = terms[0].astype(f32)
        for term in terms[1:]:
            value = value + term.astype(f32)
        return value.astype(bf16)

    my_cols = cols(seat.tp)
    y_cols = cols((1 - seat.y) * 2 + seat.c)
    core_cols = [cols(seat.y * 2 + 1 - seat.c), cols((1 - seat.y) * 2 + 1 - seat.c)]

    tail_rows = tail_ref.shape[0]
    edge = slice(tokens - tail_rows, tokens)

    def send_halo():
        loads[4].wait()
        loads[5].wait()
        tail_ref[...] = inner[edge, :].astype(f32) * given[edge, :].astype(f32)
        pl.semaphore_wait(barrier, len(peers))

        @pl.when(seat.sp < 2 * n_k - 1)
        def _():
            push(tail_ref, early, "h0", 0, seat.next_tokens(1))

    loads[0].wait()
    loads[1].wait()
    place_of = lax.broadcasted_iota(jnp.int32, (n_k, tokens), 0)
    number = jnp.zeros((n_k, tokens), jnp.int32)
    for k in range(n_k):
        number = jnp.where(place_of == k, seat.plane(k), number)
    named = [routes_ref[j:j + 1, :] == number for j in range(2)]
    member = jnp.where(named[0] | named[1], 1.0, 0.0)
    share = jnp.where(named[0], weights_ref[0:1, :], 0.0) + jnp.where(
        named[1], weights_ref[1:2, :], 0.0
    )
    sooner = lax.broadcasted_iota(jnp.int32, (tokens, tokens), 0) < lax.broadcasted_iota(
        jnp.int32, (tokens, tokens), 1
    )
    rank = jnp.dot(
        member.astype(bf16), jnp.where(sooner, 1.0, 0.0).astype(bf16), preferred_element_type=f32
    )
    slot = lax.broadcasted_iota(jnp.int32, (capacity, tokens), 0).astype(f32)
    for k in range(n_k):
        chosen = jnp.where(slot == rank[k:k + 1], member[k:k + 1], 0.0)
        slot_weight[k] = jnp.sum(chosen * share[k:k + 1], axis=1, keepdims=True)
        sel[k * capacity:(k + 1) * capacity, :] = chosen.astype(bf16)

    def pick(kind, k, span):
        got = jnp.dot(
            sel[k * capacity:(k + 1) * capacity, :], block[kind, :, span],
            preferred_element_type=f32,
        )
        if kind:
            got = got * slot_weight[k]
        return got.astype(bf16)

    order = list(range(n_k))

    def fill(k, kind):
        send[kind, k] = pick(kind, k, my_cols)

    def launch(k, kind):
        plane = seat.between(k)
        push(send.at[kind, k], places[kind].at[k, seat.x, :, my_cols], "z", (kind, k),
             (plane * 2 + seat.x, seat.tp))

    def fill_own(kind):
        for tp in range(model // width):
            span = slice(tp * width, (tp + 1) * width)
            places[kind][0, seat.x, :, span] = pick(kind, 0, span)

    def spot_of(item, x, span):
        kind, k = item
        return places[kind].at[k, x, :, span]

    def half_of(item, x, span, j):
        kind, k = item
        edge_at = capacity // 3 // 16 * 16
        part_rows = pl.ds(edge_at, capacity - edge_at) if j else pl.ds(0, edge_at)
        return places[kind].at[k, x, part_rows, span]

    ox = 1 - seat.x

    def to_core(spot, item):
        kind, k = item
        push(spot, spot, "c" if k else "c0", item if k else kind, seat.other_core())

    def s1(item):
        kind, k = item
        if k == 0:
            spot = spot_of(item, seat.x, my_cols)
            push(spot, spot, "x", item, seat.over_x())
        else:
            spot = spot_of(item, seat.x, my_cols)
            landed(spot, "z", item)
            push(spot, spot, "x", item, seat.over_x())
            push(spot, spot, "y", item, seat.over_y())
            push(spot, spot, "c", item, seat.other_core())

    def s2x(item):
        kind, k = item
        spot = spot_of(item, ox, my_cols)
        landed(spot, "x", item)
        if k == 0:
            push(spot, spot, "y", item, seat.over_y())
        else:
            part_spot = half_of(item, ox, my_cols, 0)
            push(part_spot, part_spot, "d", item, seat.over_y())
        to_core(spot, item)

    def s2y(item):
        spot = spot_of(item, seat.x, y_cols)
        landed(spot, "y", item)
        part_spot = half_of(item, seat.x, y_cols, 1)
        push(part_spot, part_spot, "d", item, seat.over_x())
        to_core(spot, item)

    def s3(item):
        kind, k = item
        spot = spot_of(item, ox, y_cols)
        if k == 0:
            landed(spot, "y", item)
        else:
            landed(spot, "d", item)
        to_core(spot, item)

    def s4(item):
        kind, k = item
        if k == 0:
            landed(rows.at[0, :, :, 0:width], "c0", kind)
        else:
            landed(rows.at[k, :, :, 0:2 * width], "c", item)

    tile = 256 if units % 256 == 0 else units

    def pre(k):
        lhs = rows[k].reshape(slots, model)
        for at in range(0, units, tile):
            gp_ref[int(k == 1), :, at:at + tile] = jnp.dot(lhs, gate[:, at:at + tile], preferred_element_type=f32)
            up_ref[int(k == 1), :, at:at + tile] = jnp.dot(lhs, up[:, at:at + tile], preferred_element_type=f32)

    def mid(k):
        lhs = cots[k].reshape(slots, model)
        for at in range(0, units, tile):
            span = slice(at, at + tile)
            grad = lax.dot_general(lhs, down[span, :], LAST, preferred_element_type=f32)
            gate_pre, up_pre = gp_ref[int(k == 1), :, span], up_ref[int(k == 1), :, span]
            sigma = jax.nn.sigmoid(gate_pre)
            silu = gate_pre * sigma
            hid[k, :, span] = (silu * up_pre).astype(bf16)
            delta[k, :, units + at:units + at + tile] = (grad * silu).astype(bf16)
            delta[k, :, span] = (grad * up_pre * sigma * (1.0 + gate_pre * (1.0 - sigma))).astype(bf16)

    def post(k, y, mine):
        out = mine_part if mine else part
        core = seat.c if mine else 1 - seat.c
        for at in range(0, width, tile):
            first = pl.ds(pl.multiple_of((y * 2 + core) * width + at, tile), tile)
            value = lax.dot_general(
                delta[k, :, :units], gate[first, :], LAST, preferred_element_type=f32
            )
            value = value + lax.dot_general(
                delta[k, :, units:], up[first, :], LAST, preferred_element_type=f32
            )
            out[k, y, :, :, at:at + tile] = value.astype(bf16).reshape(2, capacity, tile)
        if not mine:
            push(part.at[k, y], a_ref.at[k, y], "r1", k, seat.other_core())

    def r2(k):
        landed(a_ref.at[k], "r1", k)
        for y in range(2):
            acc[k, y] = total(mine_part[k, y], a_ref[k, y])
        for j, (y, x) in enumerate(((1 - seat.y, ox), (seat.y, seat.x))):
            push(acc.at[k, y, ox, pl.ds(0, cut), :], b1a.at[k, y], "r2", (k, 2 * j), seat.over_x())
            push(acc.at[k, 1 - seat.y, x, pl.ds(cut, capacity - cut), :], b1b.at[k, x], "r2",
                 (k, 2 * j + 1), seat.over_y())

    def r3(k):
        for j, (y, x) in enumerate(((1 - seat.y, ox), (seat.y, seat.x))):
            landed(b1a.at[k, y], "r2", (k, 2 * j))
            acc2a[k, y] = total(acc[k, y, seat.x, 0:cut, :], b1a[k, y])
            if j == 0:
                push(acc2a.at[k, y], b2a.at[k], "r3", (k, 0), seat.over_y())
            landed(b1b.at[k, x], "r2", (k, 2 * j + 1))
            acc2b[k, x] = total(acc[k, seat.y, x, cut:capacity, :], b1b[k, x])
            if j == 0:
                push(acc2b.at[k, x], b2b.at[k], "r3", (k, 1), seat.over_x())

    def r4(k):
        out = fin.at[k] if k else ret.at[0]
        for j, (mine, theirs) in enumerate(((acc2a, b2a), (acc2b, b2b))):
            landed(theirs.at[k], "r3", (k, j))
            span = pl.ds(cut, capacity - cut) if j else pl.ds(0, cut)
            out[span, :] = total(mine[k, seat.x if j else seat.y], theirs[k])
            if k:
                push(fin.at[k, span], ret.at[k, span], "r4", 0, seat.over_z(k))

    step = 256 if model % 256 == 0 else model
    pieces = [(0, at) for at in range(0, model, step)] + [(1, at) for at in range(0, model, 2 * step)]

    def work(count):
        for _ in range(min(count, len(pieces))):
            kind, at = pieces.pop(0)
            if kind == 0:
                lhs = rows[:, :, :, at:at + step].reshape(n_k * slots, step)
                for half in range(2):
                    out = up_grad if half else gate_grad
                    out[at:at + step, :] = lax.dot_general(
                        lhs, delta[:, :, half * units:(half + 1) * units].reshape(n_k * slots, units),
                        FIRST, preferred_element_type=f32,
                    ).astype(bf16)
            else:
                rhs = cots[:, :, :, at:at + 2 * step].reshape(n_k * slots, 2 * step)
                down_grad[:, at:at + 2 * step] = lax.dot_general(
                    hid[...].reshape(n_k * slots, units), rhs, FIRST, preferred_element_type=f32
                ).astype(bf16)

    share_rows = tokens // 2
    slice_width = g_ref.shape[4]

    def convolve():
        loads[10].wait()
        loads[9].wait()
        @pl.when(seat.sp > 0)
        def _():
            landed(early, "h0", 0)

        @pl.when(seat.sp == 0)
        def _():
            early[...] = jnp.zeros_like(early)

        earlier = early[tail_rows - 2:tail_rows, :]
        mixed = inner[...].astype(f32) * given[...].astype(f32)
        padded = jnp.concatenate([earlier, mixed], axis=0)
        t = taps[...].astype(f32)
        value = t[0:1] * padded[0:tokens] + t[1:2] * padded[1:tokens + 1]
        value = value + t[2:3] * mixed
        sum_ref[...] = value
        value = (outer[...].astype(f32) * value).astype(bf16)
        for j in range(2):
            c_ref[j, 0, 0] = value[j * share_rows:(j + 1) * share_rows]

    def spread_z():
        for k in range(1, n_k):
            push(c_ref.at[:, 0, 0], c_ref.at[:, k, 0], "cz", 0, seat.over_z(k))

    def spread_x():
        landed(c_ref.at[:, 1:n_k, 0], "cz", 0)
        for k in range(n_k):
            push(c_ref.at[:, k, 0], c_ref.at[:, k, 1], "cx", 0, seat.over_x())

    near, far, cross = 1, 2, 3
    items = [(kind, k) for k in (0, near, cross, far) for kind in range(2)]

    def away(k):
        post(k, 0, False)
        post(k, 1, False)

    def keep(k):
        post(k, 0, True)
        post(k, 1, True)

    border = late.shape[0]
    ends = [(k, s) for k in order for s in range(2) if k or s]

    def gather():
        landed(ret.at[1:n_k], "r4", 0)
        moe = lax.dot_general(
            sel[...], ret[...].reshape(n_k * capacity, width), FIRST, preferred_element_type=f32
        )
        sg[:, my_cols] = total(block[1, :, my_cols], moe.astype(bf16))
        spot = sg.at[:, my_cols]
        push(spot, spot, "ag", 0, seat.over_y())
        push(spot, spot, "ag", 1, seat.other_core())

    def flip(bits):
        number, weight = 0, 1
        while weight < n_k:
            number = number + weight * lax.rem(bits // weight + seat.tp // weight, 2)
            weight *= 2
        return number

    def g_half(k, swap, core):
        return g_ref.at[core, k, swap]

    mine_half = pl.ds(pl.multiple_of(seat.c * share_rows, share_rows), share_rows)

    def g_send(j):
        plane = flip(j)
        k = seat.between(plane)
        for s in range(2):
            d = plane * 2 + (ox if s else seat.x)
            src = sg.at[mine_half, pl.ds(pl.multiple_of(d * slice_width, slice_width), slice_width)]
            if s:
                push(src, g_half(k, s, seat.c), "g", (k, s), (d, seat.tp))
            else:
                @pl.when(k > 0)
                def _():
                    push(src, g_half(k, s, seat.c), "g", (k, s), (d, seat.tp))

    def gather_core():
        landed(sg.at[:, core_cols[0]], "ag", 1)

    def gather_y():
        spot = sg.at[:, y_cols]
        landed(spot, "ag", 0)
        push(spot, spot, "ag", 2, seat.other_core())

    def gather_rest():
        landed(sg.at[:, core_cols[1]], "ag", 2)

    def project():
        conv_grad = jnp.dot(sg[...], ow[...], preferred_element_type=f32)
        ext[0:tokens, :] = conv_grad * outer[...].astype(f32)

        @pl.when(seat.sp > 0)
        def _():
            push(ext.at[0:border, :], late, "h1", 0, seat.next_tokens(-1))

        outer_grad[...] = (conv_grad * sum_ref[...]).astype(bf16)
        own = pl.ds(pl.multiple_of(seat.sp * slice_width, slice_width), slice_width)
        for j in range(2):
            g_ref[j, 0, 0] = sg[j * share_rows:(j + 1) * share_rows, own]

    def finish_conv():
        @pl.when(seat.sp < 2 * n_k - 1)
        def _():
            landed(late, "h1", 0)
            ext[tokens:tokens + border, :] = late[...]

        @pl.when(seat.sp == 2 * n_k - 1)
        def _():
            ext[tokens:tokens + border, :] = jnp.zeros_like(late)

        t = taps[...].astype(f32)
        mixed_grad = t[2:3] * ext[0:tokens, :]
        mixed_grad = mixed_grad + t[1:2] * ext[1:tokens + 1, :]
        mixed_grad = mixed_grad + t[0:1] * ext[2:tokens + 2, :]
        inner_grad[...] = (mixed_grad * given[...].astype(f32)).astype(bf16)
        input_grad[...] = (mixed_grad * inner[...].astype(f32)).astype(bf16)

    def g_wait(k, s):
        spot = g_half(k, s, seat.c)
        landed(spot, "g", (k, s))
        push(spot, spot, "gc", 0, seat.other_core())

    def g_add(core):
        rows_of = 2 * n_k * share_rows
        return lax.dot_general(
            g_ref[core].reshape(rows_of, slice_width), c_ref[core].reshape(rows_of, -1), FIRST,
            preferred_element_type=f32,
        )

    def g_own():
        landed(c_ref.at[:, :, 1], "cx", 0)
        out_grad[...] = g_add(seat.c)

    def g_other():
        landed(sg.at[0:share_rows, 0:len(ends) * slice_width], "gc", 0)
        out_grad[...] += g_add(1 - seat.c)

    def drain():
        pieces_sent = sg.at[0:share_rows, 0:len(ends) * slice_width]
        spans = {
            "z": send.at[:, 1:n_k], "x": rows.at[:, :, :, 0:width], "y": rows.at[:, :, :, 0:width],
            "d": send.at[:, 1:n_k], "c0": rows.at[0:2, :, :, 0:width], "c": rows.at[0:n_k - 1],
            "r1": part, "r2": part.at[:, 0], "r3": part.at[:, 0, 0], "r4": part.at[0:n_k - 1, 0, 0],
            "ag": sg.at[:, 0:3 * width], "g": pieces_sent, "gc": pieces_sent,
            "cz": c_ref.at[:, 1:n_k, 0], "cx": c_ref.at[:, :, 0], "h0": tail_ref,
            "h1": ext.at[0:border, :],
        }

        def wait_sent(name):
            span, at = spans[name], names.index(name)
            remote(span, span, sent_sem.at[at], load_sem.at[0], seat.other_core()).wait_send()

        for name in names:
            if name == "h0":
                pl.when(seat.sp < 2 * n_k - 1)(functools.partial(wait_sent, name))
            elif name == "h1":
                pl.when(seat.sp > 0)(functools.partial(wait_sent, name))
            else:
                wait_sent(name)

    inner_plane = (seat.z + seat.z // 2) % 2

    def first_wave(kind):
        launch(near + inner_plane * (cross - near), kind)

        @pl.when(inner_plane == 1)
        def _():
            launch(near, kind)

    def second_wave():
        for kind in range(2):
            launch(cross - inner_plane * (cross - far), kind)

    def third_wave():
        @pl.when(inner_plane == 0)
        def _():
            for kind in range(2):
                launch(far, kind)

    loads[2].wait()
    fill(near, 0)
    fill(cross, 0)
    fill_own(0)
    send_halo()
    s1(items[0])
    first_wave(0)
    loads[3].wait()
    fill(near, 1)
    fill(cross, 1)
    first_wave(1)
    fill_own(1)
    s1(items[1])
    fill(far, 0)
    fill(far, 1)
    s1(items[2])
    s2x(items[0])
    second_wave()
    s1(items[3])
    s2y(items[2])
    third_wave()
    s2x(items[1])
    s2x(items[2])
    s2x(items[3])
    s1(items[4])
    s2y(items[3])
    s3(items[0])
    s1(items[5])
    s3(items[1])
    s4(items[0])
    s3(items[2])
    s2x(items[4])
    for load in loads[6:9]:
        load.wait()
    pre(0)
    s1(items[6])
    s2y(items[4])
    s4(items[2])
    s4(items[1])
    convolve()
    s3(items[3])
    mid(0)
    s2x(items[5])
    post(0, 1, True)
    post(0, 0, True)
    s4(items[3])
    s2y(items[5])
    post(0, 1, False)
    pre(near)
    s1(items[7])
    spread_z()
    s3(items[4])
    mid(near)
    post(0, 0, False)
    s2y(items[6])
    post(near, 1, True)
    s2x(items[6])
    s3(items[5])
    s4(items[4])
    pre(cross)
    post(near, 0, False)
    r2(0)
    post(near, 0, True)
    s2x(items[7])
    s2y(items[7])
    post(near, 1, False)
    s3(items[6])
    s4(items[5])
    mid(cross)
    post(cross, 0, True)
    post(cross, 1, False)
    r2(near)
    s4(items[6])
    post(cross, 0, False)
    pre(far)
    s3(items[7])
    post(cross, 1, True)
    r2(cross)
    s4(items[7])
    r3(0)
    mid(far)
    r3(near)
    post(far, 1, False)
    post(far, 0, False)
    post(far, 0, True)
    post(far, 1, True)
    r3(cross)
    r2(far)
    r4(0)
    r4(near)
    work(2)
    r4(cross)
    work(1)
    r3(far)
    spread_x()
    work(3)
    r4(far)
    work(3)
    gather()
    g_send(0)
    work(3)
    loads[11].wait()
    gather_core()
    g_send(1)
    work(len(pieces))
    gather_y()
    g_send(2)
    gather_rest()
    g_send(3)
    project()
    for k, s in ends:
        g_wait(k, s)
    finish_conv()
    g_own()
    g_other()
    drain()


def write_kernel(count, *refs):
    sources, targets, done = refs[:count], refs[count:2 * count], refs[2 * count]
    for n in range(count):
        rows = sources[n].shape[0]
        step = rows // 8 if rows % 128 == 0 and rows > 256 else rows
        for at in range(0, rows, step):
            span = pl.ds(at, step)
            pltpu.make_async_copy(sources[n].at[span], targets[n].at[span], done.at[n]).start()
    for n in range(count):
        pltpu.make_async_copy(sources[n], targets[n], done.at[n]).wait()


def in_vmem(count):
    return [pl.BlockSpec(memory_space=pltpu.VMEM)] * count


def in_hbm(count):
    return [pl.BlockSpec(memory_space=pltpu.HBM)] * count


def fused(cotangent, stream, routes, route_weights, gate, up, down, outer, inner, given, taps,
          out_weight, experts, capacity):
    tokens, model = stream.shape
    units = gate.shape[1]
    channels = outer.shape[1]
    width = model // 4
    slice_width = model // (2 * experts)
    border, tail_rows = min(8, tokens), min(16, tokens)
    cut = capacity // 2 // 16 * 16
    rest = capacity - cut
    bf16, f32 = jnp.bfloat16, jnp.float32
    n = experts
    slots = 2 * capacity
    gate_shape = jax.ShapeDtypeStruct((model, units), bf16)
    own = jax.ShapeDtypeStruct((tokens, channels), bf16)
    outs = (
        gate_shape, gate_shape, jax.ShapeDtypeStruct((units, model), bf16),
        jax.ShapeDtypeStruct((slice_width, channels), f32), own, own, own,
    )
    half = (n, 2, 2, capacity, width)
    scratch = [
        ((2, tokens), jnp.int32), ((2, tokens), f32), ((2, tokens, model), bf16),
        ((n * capacity, tokens), bf16), ((n, capacity, 1), f32),
        ((model, units), bf16), ((model, units), bf16), ((units, model), bf16),
        ((tokens, channels), bf16), ((tokens, channels), bf16), ((tokens, channels), bf16),
        ((3, channels), bf16), ((model, channels), bf16),
        ((2, n, capacity, width), bf16), ((n, 2, capacity, model), bf16),
        ((n, 2, capacity, model), bf16), ((2, slots, units), f32), ((2, slots, units), f32),
        ((n, slots, units), bf16), ((n, slots, 2 * units), bf16),
        (half, bf16), (half, bf16), (half, bf16), (half, bf16),
        ((n, 2, cut, width), bf16), ((n, 2, rest, width), bf16),
        ((n, 2, cut, width), bf16), ((n, 2, rest, width), bf16),
        ((n, cut, width), bf16), ((n, rest, width), bf16),
        ((n, capacity, width), bf16), ((n, capacity, width), bf16),
        ((tokens, model), bf16), ((2, n, 2, tokens // 2, slice_width), bf16),
        ((2, n, 2, tokens // 2, channels), bf16), ((tokens, channels), f32),
        ((tail_rows, channels), f32), ((tail_rows, channels), f32),
        ((tokens + border, channels), f32), ((border, channels), f32),
    ]
    sems = [pltpu.SemaphoreType.DMA((12,)), pltpu.SemaphoreType.DMA((len(SEMS),))]
    sems += [pltpu.SemaphoreType.DMA(shape_of(n)) for shape_of in SEMS.values()]
    made = pl.pallas_call(
        functools.partial(fused_kernel, experts, capacity),
        out_shape=tuple(pltpu.VMEM(out.shape, out.dtype) for out in outs),
        in_specs=in_hbm(12),
        out_specs=tuple(in_vmem(7)),
        scratch_shapes=[pltpu.VMEM(*s) for s in scratch] + sems,
        compiler_params=pltpu.CompilerParams(
            collective_id=0, has_side_effects=True, vmem_limit_bytes=48 * 1024 * 1024
        ),
        name="fused",
    )(*[
        pltpu.with_memory_space_constraint(value, pltpu.HBM)
        for value in (
            routes.T, route_weights.T, stream, cotangent, gate, up, down, outer, inner, given,
            taps, out_weight,
        )
    ])
    written = pl.pallas_call(
        functools.partial(write_kernel, len(outs)),
        out_shape=outs,
        in_specs=in_vmem(len(outs)),
        out_specs=tuple(in_hbm(len(outs))),
        scratch_shapes=[pltpu.SemaphoreType.DMA((len(outs),))],
        compiler_params=pltpu.CompilerParams(vmem_limit_bytes=1024 * 1024),
        name="write",
    )(*made)
    return tuple(out[None] for out in written[:3]) + tuple(written[3:])


def per_device(
    cotangent,
    stream,
    routes,
    route_weights,
    gate_weight,
    up_weight,
    down_weight,
    outer_gate,
    inner_gate,
    conv_input,
    conv_taps,
    out_weight,
):
    groups = lax.axis_size("sp")
    tp_count = lax.axis_size("tp")
    experts = groups // 2
    tok_rows = stream.shape[0]
    model_width = stream.shape[1]
    capacity = 3 * tok_rows // experts
    slot_total = experts * capacity
    contract_first = (((0,), (0,)), ((), ()))
    contract_last = (((1,), (1,)), ((), ()))
    block_width = model_width // tp_count
    slots = groups * capacity
    even = experts == tp_count == 4
    if even and capacity % 32 == 0 and block_width % 128 == 0:
        return fused(
            cotangent, stream, routes, route_weights, gate_weight[0], up_weight[0],
            down_weight[0], outer_gate, inner_gate, conv_input, conv_taps, out_weight,
            experts, capacity,
        )
    taps = conv_taps.astype(jnp.float32)
    outer_f = outer_gate.astype(jnp.float32)
    inner_f = inner_gate.astype(jnp.float32)
    input_f = conv_input.astype(jnp.float32)
    mixed = inner_f * input_f
    flat_routes = routes.reshape(-1)
    choose = (flat_routes[:, None] == jnp.arange(experts, dtype=jnp.int32)[None, :]).astype(
        jnp.int32
    )
    before = jnp.cumsum(choose, axis=0) - choose
    slot_place = flat_routes * capacity + jnp.sum(before * choose, axis=1)
    slot_table = (jnp.arange(slot_total, dtype=jnp.int32)[:, None] == slot_place[None, :]).astype(
        jnp.float32
    )
    select = jnp.sum(slot_table.reshape(slot_total, tok_rows, 2), axis=2).astype(jnp.bfloat16)
    slot_weight = jnp.sum(slot_table * route_weights.reshape(-1)[None, :], axis=1)
    offset = lax.axis_index("tp") * block_width
    rows_part = lax.dynamic_slice_in_dim(stream, offset, block_width, 1)
    cot_part = lax.dynamic_slice_in_dim(cotangent, offset, block_width, 1)
    sent_rows = jnp.dot(select, rows_part, preferred_element_type=jnp.float32).astype(jnp.bfloat16)
    sent_cot = (
        jnp.dot(select, cot_part, preferred_element_type=jnp.float32) * slot_weight[:, None]
    ).astype(jnp.bfloat16)
    sent_rows = jnp.repeat(sent_rows.reshape(experts, capacity, -1), 2, axis=0)
    sent_cot = jnp.repeat(sent_cot.reshape(experts, capacity, -1), 2, axis=0)
    recv_rows, recv_cot = (
        lax.all_to_all(sent_rows, "sp", split_axis=0, concat_axis=0, tiled=True),
        lax.all_to_all(sent_cot, "sp", split_axis=0, concat_axis=0, tiled=True),
    )
    recv_rows, recv_cot = (
        lax.all_gather(recv_rows, "tp", axis=2, tiled=True),
        lax.all_gather(recv_cot, "tp", axis=2, tiled=True),
    )
    routed_rows = recv_rows.reshape(slots, model_width)
    routed_cot = recv_cot.reshape(slots, model_width)
    earlier = from_behind(mixed[-2:], "sp", 1)
    gate_local = gate_weight[0]
    up_local = up_weight[0]
    down_local = down_weight[0]
    gate_pre = jnp.dot(routed_rows, gate_local, preferred_element_type=jnp.float32)
    up_pre = jnp.dot(routed_rows, up_local, preferred_element_type=jnp.float32)
    hidden_grad = lax.dot_general(
        routed_cot, down_local, contract_last, preferred_element_type=jnp.float32
    )
    sigma = jax.nn.sigmoid(gate_pre)
    silu_gate = gate_pre * sigma
    hidden = (silu_gate * up_pre).astype(jnp.bfloat16)
    up_delta = (hidden_grad * silu_gate).astype(jnp.bfloat16)
    gate_delta = (hidden_grad * up_pre * sigma * (1.0 + gate_pre * (1.0 - sigma))).astype(
        jnp.bfloat16
    )
    row_partial = lax.dot_general(
        gate_delta, gate_local, contract_last, preferred_element_type=jnp.float32
    )
    row_partial = row_partial + lax.dot_general(
        up_delta, up_local, contract_last, preferred_element_type=jnp.float32
    )
    padded = jnp.concatenate([earlier, mixed], axis=0)
    conv_sum = taps[0] * padded[:-2] + taps[1] * padded[1:-1] + taps[2] * padded[2:]
    conv_out = (outer_f * conv_sum).astype(jnp.bfloat16)
    gate_grad = lax.dot_general(
        routed_rows, gate_delta, contract_first, preferred_element_type=jnp.float32
    ).astype(jnp.bfloat16)[None]
    up_grad = lax.dot_general(
        routed_rows, up_delta, contract_first, preferred_element_type=jnp.float32
    ).astype(jnp.bfloat16)[None]
    down_grad = lax.dot_general(
        hidden, routed_cot, contract_first, preferred_element_type=jnp.float32
    ).astype(jnp.bfloat16)[None]
    half_sums = lax.psum_scatter(
        row_partial.astype(jnp.bfloat16), "tp", scatter_dimension=1, tiled=True
    ).astype(jnp.float32)
    block_width = half_sums.shape[1]
    half_grad = half_sums.reshape(groups, capacity, block_width).astype(jnp.bfloat16)
    returned = lax.all_to_all(half_grad, "sp", split_axis=0, concat_axis=0, tiled=True)
    returned = returned.reshape(experts, 2, capacity, block_width)
    select_three = select.reshape(experts, capacity, tok_rows)
    moe_part = jnp.einsum(
        "ecr,emcd->rd", select_three, returned, preferred_element_type=jnp.float32
    ).astype(jnp.bfloat16)
    moe_grad = lax.all_gather(moe_part, "tp", axis=1, tiled=True)
    stream_grad = (cotangent.astype(jnp.float32) + moe_grad.astype(jnp.float32)).astype(
        jnp.bfloat16
    )
    out_grad = lax.psum_scatter(
        lax.dot_general(
            stream_grad, conv_out, contract_first, preferred_element_type=jnp.float32
        ).astype(jnp.bfloat16),
        "sp",
        scatter_dimension=0,
        tiled=True,
    ).astype(jnp.float32)
    conv_grad = jnp.dot(stream_grad, out_weight, preferred_element_type=jnp.float32)
    outer_grad = (conv_grad * conv_sum).astype(jnp.bfloat16)
    scaled = conv_grad * outer_f
    later = from_behind(scaled[:2], "sp", -1)
    extended = jnp.concatenate([scaled, later], axis=0)
    mixed_grad = taps[2] * extended[:-2] + taps[1] * extended[1:-1] + taps[0] * extended[2:]
    inner_grad = (mixed_grad * input_f).astype(jnp.bfloat16)
    input_grad = (mixed_grad * inner_f).astype(jnp.bfloat16)
    return (gate_grad, up_grad, down_grad, out_grad, outer_grad, inner_grad, input_grad)


def solution(mesh):
    placed = (
        P("sp", None),
        P("sp", None),
        P("sp", None),
        P("sp", None),
        P("sp", None, "tp"),
        P("sp", None, "tp"),
        P("sp", "tp", None),
        P("sp", "tp"),
        P("sp", "tp"),
        P("sp", "tp"),
        P(None, "tp"),
        P(None, "tp"),
    )
    return jax.shard_map(
        per_device,
        mesh=mesh,
        in_specs=placed,
        out_specs=(
            P("sp", None, "tp"),
            P("sp", None, "tp"),
            P("sp", "tp", None),
            P("sp", "tp"),
            P("sp", "tp"),
            P("sp", "tp"),
            P("sp", "tp"),
        ),
        check_vma=False,
    )
```
